32 devices in a mesh: grp: 2 (over y), sp: 4 (over z), tp: 4 (over x, core).
Axes of the slice: x: 2, y: 2, z: 4, core: 2. Of those that a mesh axis runs over, the one named last changes fastest.
Arguments:
- inputs: bfloat16 [2048, 2048], P(('grp', 'sp')), parts along dimension 0, may hold values from -6 to 6
- norm_gain: float32 [2048], replicated, may hold values from 0.1 to 1.9
- da_query_weight: bfloat16 [2048, 1024], P('sp', 'tp'), may hold values from -0.125 to 0.125
- da_key_weight: bfloat16 [2048, 1024], P('sp', 'tp'), may hold values from -0.125 to 0.125
- da_value_weight: bfloat16 [2048, 1024], P('sp', 'tp'), may hold values from -0.125 to 0.125
- sw_query_weight: bfloat16 [2048, 1024], P('sp', 'tp'), may hold values from -0.125 to 0.125
- sw_key_weight: bfloat16 [2048, 512], P('sp', 'tp'), may hold values from -0.125 to 0.125
- sw_value_weight: bfloat16 [2048, 512], P('sp', 'tp'), may hold values from -0.125 to 0.125
- da_query_gain: float32 [64], replicated, may hold values from 0.6 to 30
- da_key_gain: float32 [64], replicated, may hold values from 0.6 to 30
- sw_query_gain: float32 [64], replicated, may hold values from 0.6 to 30
- sw_key_gain: float32 [64], replicated, may hold values from 0.6 to 30
- mix_lambda: float32 [8], P('tp'), may hold values from 0.3 to 0.8
- head_gain: float32 [128], replicated, may hold values from 0.1 to 1.9
- sink_logit: float32 [16], P('tp'), may hold values from 0 to 8
- da_out_weight: bfloat16 [1024, 2048], P('tp'), may hold values from -0.1875 to 0.1875
- sw_out_weight: bfloat16 [1024, 2048], P('tp'), may hold values from -0.1875 to 0.1875
Outputs:
- mixed: bfloat16 [2048, 2048], P(('grp', 'sp')), parts along dimension 0
The draws below stay inside these ranges and needn't reach their ends.
There are 2 independent parts, one for each index of `grp`. The reference program is written for one: setup_inputs(seed, part) draws one part's arguments, and reference() takes and returns one part's arrays. A program takes and returns all parts, laid end to end along the dimension named above; an argument that names none is the same for every part. Nothing has to cross between parts.
All inputs are finite; a program needn't handle non-finite values.
Results may differ from the reference program's by a relative error of at most 0.014.
The reference program's roundings to bfloat16 on the way count: a program that leaves them out, or rounds other values in their place, can miss the bound.
Values may be sent and summed in bfloat16 or wider, within the bound.
A program may use at most 64 MiB of HBM per device.

```python
import math
import jax
import jax.numpy as jnp
from jax import lax

D = 2048
DA_HEADS = 8
SW_HEADS = 16
KV_HEADS = 8
HD = 64
WINDOW = 128
SEQ = 1024
N_TP = 4


def gain_draw(key, own):
    values = jax.random.uniform(jax.random.fold_in(key, own), (HD,), jnp.float32, 0.6, 2.4)
    return values


def draw_da_query_gain(key, part):
    return gain_draw(key, 11)


def draw_da_key_gain(key, part):
    return gain_draw(key, 12)


def draw_sw_query_gain(key, part):
    return gain_draw(key, 13)


def draw_sw_key_gain(key, part):
    return gain_draw(key, 14)


def level_of(key, extent, cuts, smallest, top_value):
    def one(dim, shards_of):
        steps = jax.random.uniform(jax.random.fold_in(jax.random.fold_in(key, 6), dim), (shards_of,), jnp.float32, smallest / len(cuts), top_value / len(cuts))
        return jnp.repeat(jnp.exp(steps), extent[dim] // shards_of).reshape((-1,) + (1,) * (len(extent) - dim - 1))

    loudness = one(*cuts[0])
    for cut in cuts[1:]:
        loudness = loudness * one(*cut)
    return loudness


def bell_draw(key, shape, width, reach, shards=(), held_as=jnp.bfloat16):
    entries = width * jax.random.normal(key, shape, jnp.float32)
    if shards:
        entries = entries * level_of(key, shape, shards, -0.22, 0.18)
    return jnp.clip(entries, -reach, reach).astype(held_as)


def setup_inputs(seed: int = 0, part: int = 0) -> dict:
    keys = jax.random.split(jax.random.key(seed), 18)
    own_keys = jax.random.split(jax.random.fold_in(keys[17], part), 18)
    inputs = bell_draw(own_keys[0], (SEQ, D), 1.0, 6.0, ((0, 4),))
    norm_gain = jnp.clip(1.0 + 0.18 * jax.random.normal(keys[1], (D,), jnp.float32), 0.1, 1.9)
    da_query_weight = bell_draw(keys[2], (D, DA_HEADS * 2 * HD), D ** -0.5, 0.125, ((0, 4), (1, 4)))
    da_key_weight = bell_draw(keys[3], (D, DA_HEADS * 2 * HD), D ** -0.5, 0.125, ((0, 4), (1, 4)))
    da_value_weight = bell_draw(keys[4], (D, DA_HEADS * 2 * HD), D ** -0.5, 0.125, ((0, 4), (1, 4)))
    sw_query_weight = bell_draw(keys[5], (D, SW_HEADS * HD), D ** -0.5, 0.125, ((0, 4), (1, 4)))
    sw_key_weight = bell_draw(keys[6], (D, KV_HEADS * HD), D ** -0.5, 0.125, ((0, 4), (1, 4)))
    sw_value_weight = bell_draw(keys[7], (D, KV_HEADS * HD), D ** -0.5, 0.125, ((0, 4), (1, 4)))
    da_query_gain = draw_da_query_gain(jax.random.fold_in(keys[17], 71), part)
    da_key_gain = draw_da_key_gain(jax.random.fold_in(keys[17], 71), part)
    sw_query_gain = draw_sw_query_gain(jax.random.fold_in(keys[17], 71), part)
    sw_key_gain = draw_sw_key_gain(jax.random.fold_in(keys[17], 71), part)
    mix_lambda = jnp.clip(0.3 + 0.5 * jax.random.uniform(keys[12], (DA_HEADS,), jnp.float32) ** level_of(keys[12], (DA_HEADS,), ((0, 4),), -0.2, 0.2), 0.3, 0.8)
    head_gain = jnp.clip(1.0 + 0.18 * jax.random.normal(keys[13], (2 * HD,), jnp.float32), 0.1, 1.9)
    sink_logit = jnp.clip(8.0 * jax.random.uniform(keys[14], (SW_HEADS,), jnp.float32) ** level_of(keys[14], (SW_HEADS,), ((0, 4),), -0.2, 0.2), 0.0, 8.0)
    da_out_weight = bell_draw(keys[15], (DA_HEADS * 2 * HD, D), (DA_HEADS * 2 * HD) ** -0.5, 0.1875, ((0, 4),))
    sw_out_weight = bell_draw(keys[16], (SW_HEADS * HD, D), (SW_HEADS * HD) ** -0.5, 0.1875, ((0, 4),))
    return {"inputs": inputs, "norm_gain": norm_gain, "da_query_weight": da_query_weight, "da_key_weight": da_key_weight, "da_value_weight": da_value_weight, "sw_query_weight": sw_query_weight, "sw_key_weight": sw_key_weight, "sw_value_weight": sw_value_weight, "da_query_gain": da_query_gain, "da_key_gain": da_key_gain, "sw_query_gain": sw_query_gain, "sw_key_gain": sw_key_gain, "mix_lambda": mix_lambda, "head_gain": head_gain, "sink_logit": sink_logit, "da_out_weight": da_out_weight, "sw_out_weight": sw_out_weight}


def rms_norm(values, gain):
    return values * lax.rsqrt(lax.optimization_barrier(jnp.mean(values * values, axis=-1, keepdims=True)) + 1e-06) * gain

def reference(inputs, norm_gain, da_query_weight, da_key_weight, da_value_weight, sw_query_weight, sw_key_weight, sw_value_weight, da_query_gain, da_key_gain, sw_query_gain, sw_key_gain, mix_lambda, head_gain, sink_logit, da_out_weight, sw_out_weight):
    length = inputs.shape[0]
    normed = rms_norm(inputs.astype(jnp.float32), norm_gain).astype(jnp.bfloat16)

    def project(matrix):
        return jnp.dot(normed, matrix, preferred_element_type=jnp.float32)
    da_query = rms_norm(project(da_query_weight).reshape(length, DA_HEADS, 2, HD), da_query_gain).astype(jnp.bfloat16)
    da_key = rms_norm(project(da_key_weight).reshape(length, DA_HEADS, 2, HD), da_key_gain).astype(jnp.bfloat16)
    da_value = project(da_value_weight).astype(jnp.bfloat16).reshape(length, DA_HEADS, 2 * HD)
    sw_query = rms_norm(project(sw_query_weight).reshape(length, SW_HEADS, HD), sw_query_gain).astype(jnp.bfloat16)
    sw_key = rms_norm(project(sw_key_weight).reshape(length, KV_HEADS, HD), sw_key_gain).astype(jnp.bfloat16)
    sw_value = project(sw_value_weight).astype(jnp.bfloat16).reshape(length, KV_HEADS, HD)
    scale = HD ** (-0.5)
    block = math.gcd(length, 512)
    positions = jnp.arange(length, dtype=jnp.int32)
    keys_wide = da_key.astype(jnp.float32)
    values_wide = da_value.astype(jnp.float32)

    def da_block(first):
        rows = lax.dynamic_slice_in_dim(da_query, first, block, 0).astype(jnp.float32)
        scores = jnp.einsum('qhmd,khmd->hmqk', rows, keys_wide) * scale
        here = first + jnp.arange(block, dtype=jnp.int32)
        scores = jnp.where(positions[None, :] <= here[:, None], scores, -jnp.inf)
        top = lax.optimization_barrier(jnp.max(scores, axis=-1, keepdims=True))
        weights = jnp.exp(scores - top)
        total = lax.optimization_barrier(jnp.sum(weights, axis=-1))
        rounded = lax.optimization_barrier(weights.astype(jnp.bfloat16)).astype(jnp.float32)
        summed = jnp.einsum('hmqk,khe->hmqe', rounded, values_wide)
        maps = summed / total[..., None]
        blend = maps[:, 0] - mix_lambda[:, None, None] * maps[:, 1]
        return jnp.transpose(blend, (1, 0, 2))
    starts = jnp.arange(length // block, dtype=jnp.int32) * block
    blend_all = lax.map(da_block, starts).reshape(length, DA_HEADS, 2 * HD)
    da_rows = rms_norm(blend_all, head_gain).astype(jnp.bfloat16).reshape(length, DA_HEADS * 2 * HD)
    groups = SW_HEADS // KV_HEADS
    count = length // WINDOW

    def band(array):
        tiles = array.astype(jnp.float32).reshape(count, WINDOW, KV_HEADS, HD)
        earlier = jnp.concatenate([jnp.zeros_like(tiles[:1]), tiles[:-1]], axis=0)
        return jnp.concatenate([earlier, tiles], axis=1)
    key_band = band(sw_key)
    value_band = band(sw_value)
    query_tiles = sw_query.astype(jnp.float32).reshape(count, WINDOW, KV_HEADS, groups, HD)
    scores = jnp.einsum('nqhgd,nkhd->nhgqk', query_tiles, key_band) * scale
    lag = WINDOW + jnp.arange(WINDOW)[:, None] - jnp.arange(2 * WINDOW)[None, :]
    key_places = jnp.arange(count)[:, None] * WINDOW - WINDOW + jnp.arange(2 * WINDOW)[None, :]
    valid = ((lag >= 0) & (lag < WINDOW))[None] & (key_places >= 0)[:, None, :]
    scores = jnp.where(valid[:, None, None], scores, -jnp.inf)
    sink = sink_logit.reshape(KV_HEADS, groups)[None, :, :, None]
    top = jnp.maximum(lax.optimization_barrier(jnp.max(scores, axis=-1)), sink)
    weights = jnp.exp(scores - top[..., None])
    total = lax.optimization_barrier(jnp.sum(weights, axis=-1)) + jnp.exp(sink - top)
    rounded = lax.optimization_barrier(weights.astype(jnp.bfloat16)).astype(jnp.float32)
    summed = jnp.einsum('nhgqk,nkhd->nqhgd', rounded, value_band)
    sw_rows = (summed / jnp.transpose(total, (0, 3, 1, 2))[..., None]).astype(jnp.bfloat16).reshape(length, SW_HEADS * HD)
    da_cols = DA_HEADS * 2 * HD // N_TP
    sw_cols = SW_HEADS * HD // N_TP
    mixed = jnp.zeros((length, D), jnp.float32)
    for member in range(N_TP):
        partial_value = jnp.dot(da_rows[:, member * da_cols:(member + 1) * da_cols], da_out_weight[member * da_cols:(member + 1) * da_cols], preferred_element_type=jnp.float32)
        partial_value = partial_value + jnp.dot(sw_rows[:, member * sw_cols:(member + 1) * sw_cols], sw_out_weight[member * sw_cols:(member + 1) * sw_cols], preferred_element_type=jnp.float32)
        mixed = mixed + lax.optimization_barrier(partial_value.astype(jnp.bfloat16)).astype(jnp.float32)
    return mixed.astype(jnp.bfloat16)
```

```python
import functools

import jax
import jax.numpy as jnp
from jax import lax
from jax.experimental import pallas as pl
from jax.experimental.pallas import tpu as pltpu
from jax.sharding import PartitionSpec as P

HD = 64
WINDOW = 128


def shifted(value, axis, steps):
    count = lax.axis_size(axis)
    first, last = (max(0, -steps), min(count, count - steps))
    return lax.ppermute(value, axis, [(source, source + steps) for source in range(first, last)])


def rms_norm(values, gain):
    return values * lax.rsqrt(jnp.mean(values * values, axis=-1, keepdims=True) + 1e-06) * gain


def absorb(state, queries, places, keys, values, key_places):
    top, total, summed = state
    scores = jnp.einsum(
        "qhmd,khmd->hmqk", queries, keys, preferred_element_type=jnp.float32
    ) * HD ** (-0.5)
    scores = jnp.where(key_places[None, :] <= places[:, None], scores, -jnp.inf)
    new_top = jnp.maximum(top, jnp.max(scores, axis=-1))
    weights = jnp.exp(scores - new_top[..., None])
    total = jnp.sum(weights, axis=-1)
    summed = jnp.einsum(
        "hmqk,khe->hmqe", weights.astype(jnp.bfloat16), values, preferred_element_type=jnp.float32
    )
    return (new_top, total, summed)


def keep(state, queries, places, keys, values, key_places):
    return state


def diff_attention(queries, places, da_key, da_value, mix_lambda, head_gain):
    rows = queries.shape[0]
    heads = queries.shape[1]
    half = rows // 2
    fresh = (
        jnp.full((heads, 2, half), -1e30, jnp.float32),
        jnp.zeros((heads, 2, half), jnp.float32),
        jnp.zeros((heads, 2, half, 2 * HD), jnp.float32),
    )
    states = (fresh, fresh)
    start = jnp.int32(0)
    keys = lax.all_gather(da_key, "sp", axis=0, tiled=True)
    values = lax.all_gather(da_value, "sp", axis=0, tiled=True)
    key_places = jnp.arange(keys.shape[0], dtype=jnp.int32)
    updated = []
    for section in range(2):
        own_rows = queries[section * half : (section + 1) * half]
        own_places = places[section * half : (section + 1) * half]
        updated.append(
            lax.cond(
                start <= jnp.max(own_places),
                absorb,
                keep,
                states[section],
                own_rows,
                own_places,
                keys,
                values,
                key_places,
            )
        )
    states = tuple(updated)
    blended = []
    for top, total, summed in states:
        maps = summed / total[..., None]
        blended.append(maps[:, 0] - mix_lambda[:, None, None] * maps[:, 1])
    blend = jnp.transpose(jnp.concatenate(blended, axis=1), (1, 0, 2))
    return rms_norm(blend, head_gain).astype(jnp.bfloat16).reshape(rows, heads * 2 * HD)


def window_attention(sw_query, sw_key, sw_value, earlier_key, earlier_value, sink_logit, first):
    rows = sw_query.shape[0]
    sw_heads = sw_query.shape[1]
    kv_heads = sw_key.shape[1]
    groups = sw_heads // kv_heads
    count = rows // WINDOW

    def band(own, earlier_tile):
        tiles = own.reshape(count, WINDOW, kv_heads, HD)
        earlier = jnp.concatenate([earlier_tile[None], tiles[:-1]], axis=0)
        return jnp.concatenate([earlier, tiles], axis=1)

    key_band = band(sw_key, earlier_key)
    value_band = band(sw_value, earlier_value)
    query_tiles = sw_query.reshape(count, WINDOW, kv_heads, groups, HD)
    scores = jnp.einsum(
        "nqhgd,nkhd->nhgqk", query_tiles, key_band, preferred_element_type=jnp.float32
    ) * HD ** (-0.5)
    lag = WINDOW + jnp.arange(WINDOW)[:, None] - jnp.arange(2 * WINDOW)[None, :]
    key_places = (
        first + jnp.arange(count)[:, None] * WINDOW - WINDOW + jnp.arange(2 * WINDOW)[None, :]
    )
    valid = ((lag >= 0) & (lag < WINDOW))[None] & (key_places >= 0)[:, None, :]
    scores = jnp.where(valid[:, None, None], scores, -jnp.inf)
    sink = sink_logit.reshape(kv_heads, groups)[None, :, :, None]
    top = jnp.maximum(jnp.max(scores, axis=-1), sink)
    weights = jnp.exp(scores - top[..., None])
    total = jnp.sum(weights, axis=-1) + jnp.exp(sink - top)
    summed = jnp.einsum(
        "nhgqk,nkhd->nqhgd",
        weights.astype(jnp.bfloat16),
        value_band,
        preferred_element_type=jnp.float32,
    )
    return (
        (summed / jnp.transpose(total, (0, 3, 1, 2))[..., None])
        .astype(jnp.bfloat16)
        .reshape(rows, sw_heads * HD)
    )


def on_device(
    inputs,
    norm_gain,
    da_query_weight,
    da_key_weight,
    da_value_weight,
    sw_query_weight,
    sw_key_weight,
    sw_value_weight,
    da_query_gain,
    da_key_gain,
    sw_query_gain,
    sw_key_gain,
    mix_lambda,
    head_gain,
    sink_logit,
    da_out_weight,
    sw_out_weight,
):
    rows = inputs.shape[0]
    normed = rms_norm(inputs.astype(jnp.float32), norm_gain).astype(jnp.bfloat16)
    pieces = (
        lax.all_gather(da_query_weight, "sp", axis=0, tiled=True),
        lax.all_gather(da_key_weight, "sp", axis=0, tiled=True),
        lax.all_gather(da_value_weight, "sp", axis=0, tiled=True),
        lax.all_gather(sw_query_weight, "sp", axis=0, tiled=True),
        lax.all_gather(sw_key_weight, "sp", axis=0, tiled=True),
        lax.all_gather(sw_value_weight, "sp", axis=0, tiled=True),
    )
    projected = tuple(
        (jnp.dot(normed, piece, preferred_element_type=jnp.float32) for piece in pieces)
    )
    da_heads = da_query_weight.shape[1] // (2 * HD)
    sw_heads = sw_query_weight.shape[1] // HD
    kv_heads = sw_key_weight.shape[1] // HD
    da_query = rms_norm(projected[0].reshape(rows, da_heads, 2, HD), da_query_gain).astype(
        jnp.bfloat16
    )
    da_key = rms_norm(projected[1].reshape(rows, da_heads, 2, HD), da_key_gain).astype(jnp.bfloat16)
    da_value = projected[2].astype(jnp.bfloat16).reshape(rows, da_heads, 2 * HD)
    sw_query = rms_norm(projected[3].reshape(rows, sw_heads, HD), sw_query_gain).astype(
        jnp.bfloat16
    )
    sw_key = rms_norm(projected[4].reshape(rows, kv_heads, HD), sw_key_gain).astype(jnp.bfloat16)
    sw_value = projected[5].astype(jnp.bfloat16).reshape(rows, kv_heads, HD)
    place = lax.axis_index("sp")
    first = place * rows
    earlier_key, earlier_value = shifted(
        (sw_key[rows - WINDOW :], sw_value[rows - WINDOW :]), "sp", 1
    )
    sw_rows = window_attention(
        sw_query, sw_key, sw_value, earlier_key, earlier_value, sink_logit, first
    )
    places = first + jnp.arange(rows, dtype=jnp.int32)
    da_rows = diff_attention(da_query, places, da_key, da_value, mix_lambda, head_gain)
    partial_value = jnp.dot(da_rows, da_out_weight, preferred_element_type=jnp.float32) + jnp.dot(
        sw_rows, sw_out_weight, preferred_element_type=jnp.float32
    )
    return lax.psum(partial_value.astype(jnp.bfloat16), "tp")


MESH = pl.DeviceIdType.MESH
F32, BF16 = jnp.float32, jnp.bfloat16
CORES = 2


def dot(a, b):
    return jnp.dot(a, b, preferred_element_type=F32)


def dot_t(a, b):
    return lax.dot_general(a, b, (((1,), (1,)), ((), ())), preferred_element_type=F32)


def pair_norm(values, gain):
    lane = lax.broadcasted_iota(jnp.int32, values.shape, 1)
    squares = values * values
    low = jnp.sum(jnp.where(lane < HD, squares, 0.0), axis=-1, keepdims=True)
    high = jnp.sum(jnp.where(lane < HD, 0.0, squares), axis=-1, keepdims=True)
    mean = jnp.where(lane < HD, low, high) * (1.0 / HD)
    return values * lax.rsqrt(mean + 1e-06) * gain


def kernel(
    n,
    x_ref,
    w_ref,
    norm_gain_ref,
    gains_ref,
    scalars_ref,
    da_out_ref,
    sw_out_ref,
    out_ref,
    xg,
    wb,
    normed,
    query,
    kv,
    scal,
    rows_out,
    rows_in,
    part_out,
    part_in,
    sum_out,
    sum_in,
    local_sem,
    x_send,
    x_recv,
    xf_send,
    xf_recv,
    w_send,
    w_recv,
    wy_send,
    wy_recv,
    wc_send,
    wc_recv,
    own_send,
    own_recv,
    kv_send,
    kv_recv,
    sc_send,
    sc_recv,
    r_send,
    r_recv,
    p_send,
    p_recv,
    s_send,
    s_recv,
    o_send,
    o_recv,
):
    y = lax.axis_index("grp")
    z = lax.axis_index("sp")
    t = lax.axis_index("tp")
    x = t // CORES
    c = t % CORES
    peer = {"tp": x * CORES + 1 - c}
    across = {"tp": (1 - x) * CORES + c}
    beside = {"grp": 1 - y}

    def at(zz, cc):
        return {"sp": zz, "tp": x * CORES + cc}

    def remote(src, dst, send, recv, device):
        return pltpu.make_async_remote_copy(
            src_ref=src,
            dst_ref=dst,
            send_sem=send,
            recv_sem=recv,
            device_id=device,
            device_id_type=MESH,
        )

    barrier = pltpu.get_barrier_semaphore()

    def greet(device):
        pl.semaphore_signal(barrier, inc=1, device_id=device, device_id_type=MESH)

    greet(peer)
    greet(across)
    greet(beside)
    for k in range(1, n):
        for cc in range(CORES):
            greet(at(lax.rem(z + k, n), cc))
    pl.semaphore_wait(barrier, 3 + (n - 1) * CORES)

    pending = []

    def go(copy, when=None):
        if when is None:
            copy.start()
        else:
            pl.when(when)(copy.start)
        pending.append((copy, when))

    def hop(d, k):
        source = z - k if d == 0 else z + k
        source = jnp.clip(source, 0, n - 1)
        target = jnp.clip(z + 1 if d == 0 else z - 1, 0, n - 1)
        src = x_ref.at[c, x] if k == 0 else xg.at[source, x]
        return remote(
            src, xg.at[source, x], x_send.at[d, k], x_recv.at[d, k], {"sp": target}
        )

    def can_hop(d, k):
        return (z - k >= 0) & (z + 1 < n) if d == 0 else (z + k < n) & (z >= 1)

    def has(d, k):
        return z - k >= 0 if d == 0 else z + k < n

    go(hop(0, 0), can_hop(0, 0))
    go(hop(1, 0), can_hop(1, 0))

    for par in range(CORES):
        zt = CORES * c + par
        for cd in range(CORES):
            go(
                remote(
                    w_ref.at[par, y, cd],
                    wb.at[z, y, cd],
                    w_send.at[par, cd],
                    w_recv.at[z],
                    at(zt, cd),
                ),
                zt != z,
            )
    owner = c == z // CORES
    own = remote(w_ref.at[z % CORES], wb.at[z], own_send, own_recv, peer)
    go(own, owner)
    own_local = pltpu.make_async_copy(w_ref.at[z % CORES], wb.at[z], local_sem.at[0])
    pl.when(owner)(own_local.start)
    own_x = pltpu.make_async_copy(x_ref.at[c], xg.at[z], local_sem.at[1])
    own_x.start()
    sc_local = pltpu.make_async_copy(scalars_ref, scal.at[c], local_sem.at[2])
    sc_local.start()
    sc = remote(scalars_ref, scal.at[c], sc_send, sc_recv, peer)
    go(sc)

    def cross(zs):
        return remote(xg.at[zs, x], xg.at[zs, x], xf_send.at[zs], xf_recv.at[zs], across)

    def weight_direct(zs):
        return remote(wb.at[zs, y, c], wb.at[zs, y, c], w_send.at[0, 0], w_recv.at[zs], peer)

    def weight_beside(zs):
        return remote(wb.at[zs, y, c], wb.at[zs, y, c], wy_send.at[zs], wy_recv.at[zs], beside)

    def weight_core(zs, which):
        yy = y if which == 0 else 1 - y
        return remote(
            wb.at[zs, yy, c], wb.at[zs, yy, c], wc_send.at[which, zs], wc_recv.at[which, zs], peer
        )

    for k in range(1, n):
        for d in range(2):
            there = has(d, k)
            zs = jnp.clip(z - k if d == 0 else z + k, 0, n - 1)

            def arrived(zs=zs, d=d, k=k):
                remote(
                    xg.at[zs, x], xg.at[zs, x], x_send.at[d, k - 1], x_recv.at[d, k - 1], across
                ).wait_recv()

            pl.when(there)(arrived)
            if k < n - 1:
                go(hop(d, k), can_hop(d, k))
            go(cross(zs), there)
        for d in range(2):
            there = has(d, k)
            zs = jnp.clip(z - k if d == 0 else z + k, 0, n - 1)
            pl.when(there)(lambda zs=zs: weight_direct(zs).wait_recv())
            go(weight_beside(zs), there)
            go(weight_core(zs, 0), there)
    others = [lax.rem(z + k, n) for k in range(1, n)]
    for zs in others:
        remote(wb.at[zs, 1 - y, c], wb.at[zs, 1 - y, c], wy_send.at[zs], wy_recv.at[zs], beside).wait_recv()
        go(weight_core(zs, 1))
    for zs in others:
        remote(
            xg.at[zs, 1 - x], xg.at[zs, 1 - x], xf_send.at[zs], xf_recv.at[zs], across
        ).wait_recv()
    own_x.wait()

    part = xg.shape[2]
    tile = 2 * part
    for i in range(n):
        for h in range(2):
            values = xg[i, h].astype(F32)
            values = rms_norm(values, norm_gain_ref[...])
            normed[i, h * part : (h + 1) * part, :] = values.astype(BF16)

    pl.when(owner)(own_local.wait)
    pl.when(jnp.logical_not(owner))(own.wait_recv)
    for zs in others:
        for which in range(2):
            yy = y if which == 0 else 1 - y
            remote(
                wb.at[zs, yy, 1 - c],
                wb.at[zs, yy, 1 - c],
                wc_send.at[which, zs],
                wc_recv.at[which, zs],
                peer,
            ).wait_recv()

    depth = wb.shape[1] * wb.shape[2] * wb.shape[3]
    wide = 2 * HD
    width = wb.shape[4]
    for i in range(n):
        acc = dot(normed[i, :, 0:depth], wb[0].reshape(depth, width))
        for j in range(1, n):
            acc += dot(normed[i, :, j * depth : (j + 1) * depth], wb[j].reshape(depth, width))
        da_q = pair_norm(acc[:, 0:wide], gains_ref[0:1, :]).astype(BF16)
        da_k = pair_norm(acc[:, wide : 2 * wide], gains_ref[1:2, :]).astype(BF16)
        da_v = acc[:, 2 * wide : 3 * wide].astype(BF16)
        sw_q = pair_norm(acc[:, 3 * wide : 4 * wide], gains_ref[2:3, :]).astype(BF16)
        sw_kv = acc[:, 4 * wide : 5 * wide]
        lane = lax.broadcasted_iota(jnp.int32, sw_kv.shape, 1)
        sw_kv = jnp.where(lane < HD, pair_norm(sw_kv, gains_ref[3:4, :]), sw_kv).astype(BF16)
        scale = jnp.asarray(HD ** (-0.5), BF16)
        query[i, :, 0:wide] = da_q * scale
        query[i, :, wide : 2 * wide] = sw_q * scale
        kv[c, i, :, 0:wide] = da_k
        kv[c, i, :, wide : 2 * wide] = da_v
        kv[c, i, :, 2 * wide : 3 * wide] = sw_kv

    swap = remote(kv.at[c], kv.at[c], kv_send, kv_recv, peer)
    go(swap)
    sc_local.wait()
    remote(scal.at[1 - c], scal.at[1 - c], sc_send, sc_recv, peer).wait_recv()
    remote(kv.at[1 - c], kv.at[1 - c], kv_send, kv_recv, peer).wait_recv()

    mine = scal[z // CORES, z % CORES]
    mix = mine[0:1, :]
    for i in range(n):
        q_place = (2 * i + c) * tile + lax.broadcasted_iota(jnp.int32, (tile, 1), 0)
        count = (i + 1) * tile
        column = lax.broadcasted_iota(jnp.int32, (1, count), 1)
        maps = []
        for m in range(2):
            q = query[i, :, m * HD : (m + 1) * HD]
            scores = []
            for h in range(2):
                keys = kv[h, 0 : i + 1, :, m * HD : (m + 1) * HD].reshape(count, HD)
                place = (column // tile) * (2 * tile) + h * tile + column % tile
                scores.append(jnp.where(place <= q_place, dot_t(q, keys), -jnp.inf))
            top = jnp.maximum(
                jnp.max(scores[0], axis=-1, keepdims=True),
                jnp.max(scores[1], axis=-1, keepdims=True),
            )
            total = 0.0
            summed = 0.0
            for h in range(2):
                weights = jnp.exp(scores[h] - top)
                total += jnp.sum(weights, axis=-1, keepdims=True)
                values = kv[h, 0 : i + 1, :, wide : 2 * wide].reshape(count, wide)
                summed += dot(weights.astype(BF16), values)
            maps.append(summed / total)
        blend = maps[0] - mix * maps[1]
        rows_out[i, :, 0:wide] = rms_norm(blend, gains_ref[4:5, :]).astype(BF16)

        before = jnp.maximum(i - 1 + c, 0)
        q_row = lax.broadcasted_iota(jnp.int32, (tile, tile), 0)
        k_row = lax.broadcasted_iota(jnp.int32, (tile, tile), 1)
        first_ok = (2 * i + c) > 0
        near = kv[c, i, :, 2 * wide : 3 * wide]
        far = kv[1 - c, before, :, 2 * wide : 3 * wide]
        results = []
        for g in range(2):
            q = query[i, :, wide + g * HD : wide + (g + 1) * HD]
            s_near = jnp.where(k_row <= q_row, dot_t(q, near[:, 0:HD]), -jnp.inf)
            s_far = jnp.where((k_row > q_row) & first_ok, dot_t(q, far[:, 0:HD]), -jnp.inf)
            sink = mine[1 + g : 2 + g, 0:1]
            top = jnp.maximum(
                jnp.max(s_near, axis=-1, keepdims=True), jnp.max(s_far, axis=-1, keepdims=True)
            )
            top = jnp.maximum(top, sink)
            w_near = jnp.exp(s_near - top)
            w_far = jnp.exp(s_far - top)
            total = (
                jnp.sum(w_near, axis=-1, keepdims=True)
                + jnp.sum(w_far, axis=-1, keepdims=True)
                + jnp.exp(sink - top)
            )
            summed = dot(w_near.astype(BF16), near[:, HD:wide]) + dot(
                w_far.astype(BF16), far[:, HD:wide]
            )
            results.append(summed / total)
        rows_out[i, :, wide : 2 * wide] = jnp.concatenate(results, axis=-1).astype(BF16)

        away = (z != i) | jnp.logical_not(owner)
        go(
            remote(
                rows_out.at[i],
                rows_in.at[z % CORES, c],
                r_send.at[i],
                r_recv.at[z % CORES, c],
                at(i, z // CORES),
            ),
            away,
        )
    keep_rows = pltpu.make_async_copy(rows_out.at[z], rows_in.at[z % CORES, c], local_sem.at[3])
    pl.when(owner)(keep_rows.start)
    pl.when(owner)(keep_rows.wait)

    def await_rows(cc):
        for par in range(CORES):

            def wait(par=par):
                remote(
                    rows_in.at[par, cc], rows_in.at[par, cc], r_send.at[0], r_recv.at[par, cc], peer
                ).wait_recv()

            pl.when((CORES * c + par != z) | (cc != c))(wait)

    columns = part_out.shape[1] // 4

    def project(cc, q):
        cols = slice(q * columns, (q + 1) * columns)
        acc = 0.0
        for par in range(CORES):
            rows = rows_in[par, cc]
            acc += dot(rows[:, 0:wide], da_out_ref[par * wide : (par + 1) * wide, cols])
            acc += dot(rows[:, wide : 2 * wide], sw_out_ref[par * wide : (par + 1) * wide, cols])
        return acc.astype(BF16)

    await_rows(1 - c)
    for q in range(4):
        part_out[:, q * columns : (q + 1) * columns] = project(1 - c, q)
        cols = pl.ds(q * columns, columns)
        go(remote(part_out.at[:, cols], part_in.at[:, cols], p_send.at[q], p_recv.at[q], peer))
    await_rows(c)
    for q in range(4):
        cols = pl.ds(q * columns, columns)
        mine_part = project(c, q).astype(F32)
        remote(part_out.at[:, cols], part_in.at[:, cols], p_send.at[q], p_recv.at[q], peer).wait_recv()
        both = mine_part + part_in[:, cols].astype(F32)
        sum_out[:, cols] = both.astype(BF16)
        go(remote(sum_out.at[:, cols], sum_in.at[:, cols], s_send.at[q], s_recv.at[q], across))
    for q in range(4):
        cols = pl.ds(q * columns, columns)
        remote(sum_out.at[:, cols], sum_in.at[:, cols], s_send.at[q], s_recv.at[q], across).wait_recv()
        total = sum_out[:, cols].astype(F32) + sum_in[:, cols].astype(F32)
        out_ref[c, :, cols] = total.astype(BF16)
        go(
            remote(
                out_ref.at[c, :, cols], out_ref.at[c, :, cols], o_send.at[q], o_recv.at[q], peer
            )
        )
    for q in range(4):
        cols = pl.ds(q * columns, columns)
        remote(
            out_ref.at[1 - c, :, cols], out_ref.at[1 - c, :, cols], o_send.at[q], o_recv.at[q], peer
        ).wait_recv()
    for copy, when in pending:
        if when is None:
            copy.wait_send()
        else:
            pl.when(when)(copy.wait_send)


def transposed(n, *arrays):
    (
        inputs,
        norm_gain,
        da_query_weight,
        da_key_weight,
        da_value_weight,
        sw_query_weight,
        sw_key_weight,
        sw_value_weight,
        da_query_gain,
        da_key_gain,
        sw_query_gain,
        sw_key_gain,
        mix_lambda,
        head_gain,
        sink_logit,
        da_out_weight,
        sw_out_weight,
    ) = arrays
    rows, d = inputs.shape
    depth = da_query_weight.shape[0]
    wide = 2 * HD
    packed = []
    for par in range(CORES):
        big = slice(par * wide, (par + 1) * wide)
        small = slice(par * HD, (par + 1) * HD)
        packed.append(
            jnp.concatenate(
                [
                    da_query_weight[:, big],
                    da_key_weight[:, big],
                    da_value_weight[:, big],
                    sw_query_weight[:, big],
                    sw_key_weight[:, small],
                    sw_value_weight[:, small],
                ],
                axis=1,
            )
        )
    width = packed[0].shape[1]
    piece = depth // 4
    weights = jnp.stack(packed).reshape(CORES, 2, CORES, piece, width)
    gains = jnp.stack(
        [
            jnp.tile(da_query_gain, 2),
            jnp.tile(da_key_gain, 2),
            jnp.tile(sw_query_gain, 2),
            jnp.tile(sw_key_gain, 2),
            head_gain,
            head_gain,
            head_gain,
            head_gain,
        ]
    )
    sinks = sink_logit.reshape(CORES, 2)
    scalars = jnp.concatenate([mix_lambda.reshape(CORES, 1), sinks, jnp.zeros((CORES, 5), F32)], axis=1)
    scalars = jnp.broadcast_to(scalars[:, :, None], (CORES, 8, wide))
    part = rows // 4
    tile = rows // 2
    DMA = pltpu.SemaphoreType.DMA
    vmem = pl.BlockSpec(memory_space=pltpu.VMEM)
    out = pl.pallas_call(
        functools.partial(kernel, n),
        out_shape=jax.ShapeDtypeStruct((2, tile, d), BF16),
        in_specs=[vmem] * 7,
        out_specs=vmem,
        scratch_shapes=[
            pltpu.VMEM((n, 2, part, d), BF16),
            pltpu.VMEM((n, 2, CORES, piece, width), BF16),
            pltpu.VMEM((n, tile, d), BF16),
            pltpu.VMEM((n, tile, 2 * wide), BF16),
            pltpu.VMEM((2, n, tile, 3 * wide), BF16),
            pltpu.VMEM((CORES, CORES, 8, wide), F32),
            pltpu.VMEM((n, tile, 2 * wide), BF16),
            pltpu.VMEM((CORES, CORES, tile, 2 * wide), BF16),
            pltpu.VMEM((tile, d), BF16),
            pltpu.VMEM((tile, d), BF16),
            pltpu.VMEM((tile, d), BF16),
            pltpu.VMEM((tile, d), BF16),
            DMA((4,)),
            DMA((2, n)),
            DMA((2, n)),
            DMA((n,)),
            DMA((n,)),
            DMA((CORES, CORES)),
            DMA((n,)),
            DMA((n,)),
            DMA((n,)),
            DMA((2, n)),
            DMA((2, n)),
            DMA,
            DMA,
            DMA,
            DMA,
            DMA,
            DMA,
            DMA((n,)),
            DMA((CORES, CORES)),
            DMA((4,)),
            DMA((4,)),
            DMA((4,)),
            DMA((4,)),
            DMA((4,)),
            DMA((4,)),
        ],
        compiler_params=pltpu.CompilerParams(
            collective_id=0, has_side_effects=True, vmem_limit_bytes=60 * 1024 * 1024
        ),
    )(
        inputs.reshape(CORES, 2, part, d),
        weights,
        norm_gain.reshape(1, d),
        gains,
        scalars,
        da_out_weight,
        sw_out_weight,
    )
    return out.reshape(rows, d)


def body(sizes, *arrays):
    rows = arrays[0].shape[0]
    heads = arrays[12].shape[0]
    sinks = arrays[14].shape[0]
    n = sizes["sp"]
    fits = (
        sizes["grp"] == 2
        and sizes["tp"] == 2 * CORES
        and n == 2 * CORES
        and heads == CORES
        and sinks == 2 * CORES
        and arrays[6].shape[1] == CORES * HD
        and rows == 2 * WINDOW
    )
    if fits:
        return transposed(n, *arrays)
    return on_device(*arrays)


def solution(mesh):
    return jax.shard_map(
        functools.partial(body, dict(mesh.shape)),
        mesh=mesh,
        in_specs=(
            P(("grp", "sp"), None),
            P(),
            P("sp", "tp"),
            P("sp", "tp"),
            P("sp", "tp"),
            P("sp", "tp"),
            P("sp", "tp"),
            P("sp", "tp"),
            P(),
            P(),
            P(),
            P(),
            P("tp"),
            P(),
            P("tp"),
            P("tp", None),
            P("tp", None),
        ),
        out_specs=P(("grp", "sp"), None),
        check_vma=False,
    )
```

```python
import functools

import jax
import jax.numpy as jnp
from jax import lax
from jax.experimental import pallas as pl
from jax.experimental.pallas import tpu as pltpu
from jax.sharding import PartitionSpec as P

HD = 64
WINDOW = 128


def shifted(value, axis, steps):
    count = lax.axis_size(axis)
    first, last = (max(0, -steps), min(count, count - steps))
    return lax.ppermute(value, axis, [(source, source + steps) for source in range(first, last)])


def rms_norm(values, gain):
    return values * lax.rsqrt(jnp.mean(values * values, axis=-1, keepdims=True) + 1e-06) * gain


def absorb(state, queries, places, keys, values, key_places):
    top, total, summed = state
    scores = jnp.einsum(
        "qhmd,khmd->hmqk", queries, keys, preferred_element_type=jnp.float32
    ) * HD ** (-0.5)
    scores = jnp.where(key_places[None, :] <= places[:, None], scores, -jnp.inf)
    new_top = jnp.maximum(top, jnp.max(scores, axis=-1))
    weights = jnp.exp(scores - new_top[..., None])
    total = jnp.sum(weights, axis=-1)
    summed = jnp.einsum(
        "hmqk,khe->hmqe", weights.astype(jnp.bfloat16), values, preferred_element_type=jnp.float32
    )
    return (new_top, total, summed)


def keep(state, queries, places, keys, values, key_places):
    return state


def diff_attention(queries, places, da_key, da_value, mix_lambda, head_gain):
    rows = queries.shape[0]
    heads = queries.shape[1]
    half = rows // 2
    fresh = (
        jnp.full((heads, 2, half), -1e30, jnp.float32),
        jnp.zeros((heads, 2, half), jnp.float32),
        jnp.zeros((heads, 2, half, 2 * HD), jnp.float32),
    )
    states = (fresh, fresh)
    start = jnp.int32(0)
    keys = lax.all_gather(da_key, "sp", axis=0, tiled=True)
    values = lax.all_gather(da_value, "sp", axis=0, tiled=True)
    key_places = jnp.arange(keys.shape[0], dtype=jnp.int32)
    updated = []
    for section in range(2):
        own_rows = queries[section * half : (section + 1) * half]
        own_places = places[section * half : (section + 1) * half]
        updated.append(
            lax.cond(
                start <= jnp.max(own_places),
                absorb,
                keep,
                states[section],
                own_rows,
                own_places,
                keys,
                values,
                key_places,
            )
        )
    states = tuple(updated)
    blended = []
    for top, total, summed in states:
        maps = summed / total[..., None]
        blended.append(maps[:, 0] - mix_lambda[:, None, None] * maps[:, 1])
    blend = jnp.transpose(jnp.concatenate(blended, axis=1), (1, 0, 2))
    return rms_norm(blend, head_gain).astype(jnp.bfloat16).reshape(rows, heads * 2 * HD)


def window_attention(sw_query, sw_key, sw_value, earlier_key, earlier_value, sink_logit, first):
    rows = sw_query.shape[0]
    sw_heads = sw_query.shape[1]
    kv_heads = sw_key.shape[1]
    groups = sw_heads // kv_heads
    count = rows // WINDOW

    def band(own, earlier_tile):
        tiles = own.reshape(count, WINDOW, kv_heads, HD)
        earlier = jnp.concatenate([earlier_tile[None], tiles[:-1]], axis=0)
        return jnp.concatenate([earlier, tiles], axis=1)

    key_band = band(sw_key, earlier_key)
    value_band = band(sw_value, earlier_value)
    query_tiles = sw_query.reshape(count, WINDOW, kv_heads, groups, HD)
    scores = jnp.einsum(
        "nqhgd,nkhd->nhgqk", query_tiles, key_band, preferred_element_type=jnp.float32
    ) * HD ** (-0.5)
    lag = WINDOW + jnp.arange(WINDOW)[:, None] - jnp.arange(2 * WINDOW)[None, :]
    key_places = (
        first + jnp.arange(count)[:, None] * WINDOW - WINDOW + jnp.arange(2 * WINDOW)[None, :]
    )
    valid = ((lag >= 0) & (lag < WINDOW))[None] & (key_places >= 0)[:, None, :]
    scores = jnp.where(valid[:, None, None], scores, -jnp.inf)
    sink = sink_logit.reshape(kv_heads, groups)[None, :, :, None]
    top = jnp.maximum(jnp.max(scores, axis=-1), sink)
    weights = jnp.exp(scores - top[..., None])
    total = jnp.sum(weights, axis=-1) + jnp.exp(sink - top)
    summed = jnp.einsum(
        "nhgqk,nkhd->nqhgd",
        weights.astype(jnp.bfloat16),
        value_band,
        preferred_element_type=jnp.float32,
    )
    return (
        (summed / jnp.transpose(total, (0, 3, 1, 2))[..., None])
        .astype(jnp.bfloat16)
        .reshape(rows, sw_heads * HD)
    )


def on_device(
    inputs,
    norm_gain,
    da_query_weight,
    da_key_weight,
    da_value_weight,
    sw_query_weight,
    sw_key_weight,
    sw_value_weight,
    da_query_gain,
    da_key_gain,
    sw_query_gain,
    sw_key_gain,
    mix_lambda,
    head_gain,
    sink_logit,
    da_out_weight,
    sw_out_weight,
):
    rows = inputs.shape[0]
    normed = rms_norm(inputs.astype(jnp.float32), norm_gain).astype(jnp.bfloat16)
    pieces = (
        lax.all_gather(da_query_weight, "sp", axis=0, tiled=True),
        lax.all_gather(da_key_weight, "sp", axis=0, tiled=True),
        lax.all_gather(da_value_weight, "sp", axis=0, tiled=True),
        lax.all_gather(sw_query_weight, "sp", axis=0, tiled=True),
        lax.all_gather(sw_key_weight, "sp", axis=0, tiled=True),
        lax.all_gather(sw_value_weight, "sp", axis=0, tiled=True),
    )
    projected = tuple(
        (jnp.dot(normed, piece, preferred_element_type=jnp.float32) for piece in pieces)
    )
    da_heads = da_query_weight.shape[1] // (2 * HD)
    sw_heads = sw_query_weight.shape[1] // HD
    kv_heads = sw_key_weight.shape[1] // HD
    da_query = rms_norm(projected[0].reshape(rows, da_heads, 2, HD), da_query_gain).astype(
        jnp.bfloat16
    )
    da_key = rms_norm(projected[1].reshape(rows, da_heads, 2, HD), da_key_gain).astype(jnp.bfloat16)
    da_value = projected[2].astype(jnp.bfloat16).reshape(rows, da_heads, 2 * HD)
    sw_query = rms_norm(projected[3].reshape(rows, sw_heads, HD), sw_query_gain).astype(
        jnp.bfloat16
    )
    sw_key = rms_norm(projected[4].reshape(rows, kv_heads, HD), sw_key_gain).astype(jnp.bfloat16)
    sw_value = projected[5].astype(jnp.bfloat16).reshape(rows, kv_heads, HD)
    place = lax.axis_index("sp")
    first = place * rows
    earlier_key, earlier_value = shifted(
        (sw_key[rows - WINDOW :], sw_value[rows - WINDOW :]), "sp", 1
    )
    sw_rows = window_attention(
        sw_query, sw_key, sw_value, earlier_key, earlier_value, sink_logit, first
    )
    places = first + jnp.arange(rows, dtype=jnp.int32)
    da_rows = diff_attention(da_query, places, da_key, da_value, mix_lambda, head_gain)
    partial_value = jnp.dot(da_rows, da_out_weight, preferred_element_type=jnp.float32) + jnp.dot(
        sw_rows, sw_out_weight, preferred_element_type=jnp.float32
    )
    return lax.psum(partial_value.astype(jnp.bfloat16), "tp")


MESH = pl.DeviceIdType.MESH
F32, BF16 = jnp.float32, jnp.bfloat16
CORES = 2


def dot(a, b):
    return jnp.dot(a, b, preferred_element_type=F32)


def dot_t(a, b):
    return lax.dot_general(a, b, (((1,), (1,)), ((), ())), preferred_element_type=F32)


def pair_norm(values, gain):
    lane = lax.broadcasted_iota(jnp.int32, values.shape, 1)
    squares = values * values
    low = jnp.sum(jnp.where(lane < HD, squares, 0.0), axis=-1, keepdims=True)
    high = jnp.sum(jnp.where(lane < HD, 0.0, squares), axis=-1, keepdims=True)
    mean = jnp.where(lane < HD, low, high) * (1.0 / HD)
    return values * lax.rsqrt(mean + 1e-06) * gain


def kernel(
    n,
    x_ref,
    da_q_ref,
    da_k_ref,
    da_v_ref,
    sw_q_ref,
    sw_k_ref,
    sw_v_ref,
    norm_gain_ref,
    da_q_gain_ref,
    da_k_gain_ref,
    sw_q_gain_ref,
    sw_k_gain_ref,
    head_gain_ref,
    mix_ref,
    sink_ref,
    da_out_hbm,
    sw_out_hbm,
    out_ref,
    da_out_ref,
    sw_out_ref,
    small,
    gains_ref,
    xg,
    wb,
    normed,
    query,
    kv,
    scal,
    rows_out,
    rows_in,
    part_out,
    part_in,
    sum_out,
    sum_in,
    local_sem,
    x_send,
    x_recv,
    xf_send,
    xf_recv,
    w_send,
    w_recv,
    wy_send,
    wy_recv,
    wc_send,
    wc_recv,
    own_send,
    own_recv,
    kv_send,
    kv_recv,
    sc_send,
    sc_recv,
    r_send,
    r_recv,
    p_send,
    p_recv,
    s_send,
    s_recv,
    o_send,
    o_recv,
):
    y = lax.axis_index("grp")
    z = lax.axis_index("sp")
    t = lax.axis_index("tp")
    x = t // CORES
    c = t % CORES
    peer = {"tp": x * CORES + 1 - c}
    across = {"tp": (1 - x) * CORES + c}
    beside = {"grp": 1 - y}

    def at(zz, cc):
        return {"sp": zz, "tp": x * CORES + cc}

    def remote(src, dst, send, recv, device):
        return pltpu.make_async_remote_copy(
            src_ref=src,
            dst_ref=dst,
            send_sem=send,
            recv_sem=recv,
            device_id=device,
            device_id_type=MESH,
        )

    barrier = pltpu.get_barrier_semaphore()

    def greet(device):
        pl.semaphore_signal(barrier, inc=1, device_id=device, device_id_type=MESH)

    greet(peer)
    greet(across)
    greet(beside)
    for k in range(1, n):
        for cc in range(CORES):
            greet(at(lax.rem(z + k, n), cc))

    own_x = pltpu.make_async_copy(x_ref.at[c], xg.at[z], local_sem.at[1])
    own_x.start()
    out_loads = [
        pltpu.make_async_copy(da_out_hbm, da_out_ref, local_sem.at[4]),
        pltpu.make_async_copy(sw_out_hbm, sw_out_ref, local_sem.at[5]),
    ]
    for load in out_loads:
        load.start()

    wide = 2 * HD
    for par in range(CORES):
        cols = slice(par * HD, (par + 1) * HD)
        small[par] = jnp.concatenate([sw_k_ref[..., cols], sw_v_ref[..., cols]], axis=-1)
        scal[c, par, 0:1, :] = jnp.broadcast_to(mix_ref[:, par : par + 1], (1, wide))
        for g in range(2):
            sink = sink_ref[:, 2 * par + g : 2 * par + g + 1]
            scal[c, par, 1 + g : 2 + g, :] = jnp.broadcast_to(sink, (1, wide))
    for i, ref in enumerate((da_q_gain_ref, da_k_gain_ref, sw_q_gain_ref, sw_k_gain_ref)):
        gains_ref[i : i + 1, :] = jnp.concatenate([ref[...], ref[...]], axis=-1)
    gains_ref[4:5, :] = head_gain_ref[...]
    pl.semaphore_wait(barrier, 3 + (n - 1) * CORES)

    pending = []

    def go(copy, when=None):
        if when is None:
            copy.start()
        else:
            pl.when(when)(copy.start)
        pending.append((copy, when))

    pieces = xg.shape[2]

    def hop(d, k, p):
        source = z - k if d == 0 else z + k
        source = jnp.clip(source, 0, n - 1)
        target = jnp.clip(z + 1 if d == 0 else z - 1, 0, n - 1)
        src = x_ref.at[c, x, p] if k == 0 else xg.at[source, x, p]
        return remote(
            src, xg.at[source, x, p], x_send.at[d, k, p], x_recv.at[d, k, p], {"sp": target}
        )

    def can_hop(d, k):
        return (z - k >= 0) & (z + 1 < n) if d == 0 else (z + k < n) & (z >= 1)

    def has(d, k):
        return z - k >= 0 if d == 0 else z + k < n

    def from_there(d, k):
        return jnp.clip(z - k if d == 0 else z + k, 0, n - 1)

    for p in range(pieces):
        for d in range(2):
            go(hop(d, 0, p), can_hop(d, 0))

    owner = c == z // CORES

    def columns_of(par, yy, cc):
        found = [
            ref.at[yy, cc, :, pl.ds(pl.multiple_of(par * wide, wide), wide)]
            for ref in (da_q_ref, da_k_ref, da_v_ref, sw_q_ref)
        ]
        return found + [small.at[par, yy, cc]]

    def own_copies(kind):
        copies = []
        for yy in range(2):
            for cc in range(CORES):
                for j, src in enumerate(columns_of(z % CORES, yy, cc)):
                    dst = wb.at[z, yy, cc, :, pl.ds(j * wide, wide)]
                    if kind == 0:
                        copies.append(pltpu.make_async_copy(src, dst, local_sem.at[0]))
                    else:
                        copies.append(remote(src, dst, own_send, own_recv, peer))
        return copies

    own = remote(wb.at[z], wb.at[z], own_send, own_recv, peer)
    own_local = pltpu.make_async_copy(wb.at[z], wb.at[z], local_sem.at[0])

    @pl.when(owner)
    def _():
        for copy in own_copies(0) + own_copies(1):
            copy.start()

    pending.append((own, owner))
    sc = remote(scal.at[c], scal.at[c], sc_send, sc_recv, peer)
    go(sc)

    def cross(zs, p):
        return remote(
            xg.at[zs, x, p], xg.at[zs, x, p], xf_send.at[zs, p], xf_recv.at[zs, p], across
        )

    def weight_direct(zs, par=0, cd=0):
        return remote(
            wb.at[zs, y, c], wb.at[zs, y, c], w_send.at[par, cd], w_recv.at[zs], peer
        )

    def weight_beside(zs):
        return remote(wb.at[zs, y, c], wb.at[zs, y, c], wy_send.at[zs], wy_recv.at[zs], beside)

    def weight_core(zs, which):
        yy = y if which == 0 else 1 - y
        return remote(
            wb.at[zs, yy, c], wb.at[zs, yy, c], wc_send.at[which, zs], wc_recv.at[which, zs], peer
        )

    def pass_on(k):
        for p in range(pieces):
            for d in range(2):
                zs = from_there(d, k)

                def arrived(zs=zs, d=d, p=p):
                    remote(
                        xg.at[zs, x, p],
                        xg.at[zs, x, p],
                        x_send.at[d, k - 1, p],
                        x_recv.at[d, k - 1, p],
                        across,
                    ).wait_recv()

                pl.when(has(d, k))(arrived)
                if k < n - 1:
                    go(hop(d, k, p), can_hop(d, k))
                go(cross(zs, p), has(d, k))

    def send_weights():
        for par in range(CORES):
            zt = CORES * c + par
            for cd in range(CORES):

                @pl.when(zt != z)
                def _(par=par, cd=cd, zt=zt):
                    for j, src in enumerate(columns_of(par, y, cd)):
                        remote(
                            src,
                            wb.at[z, y, cd, :, pl.ds(j * wide, wide)],
                            w_send.at[par, cd],
                            w_recv.at[z],
                            at(zt, cd),
                        ).start()

                pending.append((weight_direct(z, par, cd), zt != z))

    def pass_weights(k):
        for d in range(2):
            zs = from_there(d, k)
            pl.when(has(d, k))(lambda zs=zs: weight_direct(zs).wait_recv())
            go(weight_beside(zs), has(d, k))
            go(weight_core(zs, 0), has(d, k))

    part = xg.shape[2] * xg.shape[3]
    tile = 2 * part

    def norm_of(i):
        for h in range(2):
            values = xg[i, h].reshape(part, xg.shape[4]).astype(F32)
            values = rms_norm(values, norm_gain_ref[...])
            normed[i, h * part : (h + 1) * part, :] = values.astype(BF16)

    pass_on(1)
    send_weights()
    pass_on(2)
    pass_weights(1)
    pass_weights(2)
    own_x.wait()
    norm_of(z)
    pass_on(3)
    pass_weights(3)
    others = [lax.rem(z + k, n) for k in range(1, n)]
    for k in range(1, n):
        for d in range(2):
            zs = from_there(d, k)

            @pl.when(has(d, k))
            def _(zs=zs):
                remote(
                    wb.at[zs, 1 - y, c],
                    wb.at[zs, 1 - y, c],
                    wy_send.at[zs],
                    wy_recv.at[zs],
                    beside,
                ).wait_recv()

            go(weight_core(zs, 1), has(d, k))
    for k in range(1, n):
        for d in range(2):

            @pl.when(has(d, k))
            def _(zs=from_there(d, k)):
                for p in range(pieces):
                    remote(
                        xg.at[zs, 1 - x, p],
                        xg.at[zs, 1 - x, p],
                        xf_send.at[zs, p],
                        xf_recv.at[zs, p],
                        across,
                    ).wait_recv()
                norm_of(zs)

    pl.when(owner)(own_local.wait)
    pl.when(jnp.logical_not(owner))(own.wait_recv)
    for zs in others:
        for which in range(2):
            yy = y if which == 0 else 1 - y
            remote(
                wb.at[zs, yy, 1 - c],
                wb.at[zs, yy, 1 - c],
                wc_send.at[which, zs],
                wc_recv.at[which, zs],
                peer,
            ).wait_recv()

    depth = wb.shape[1] * wb.shape[2] * wb.shape[3]
    width = wb.shape[4]
    for i in range(n):
        acc = dot(normed[i, :, 0:depth], wb[0].reshape(depth, width))
        for j in range(1, n):
            acc += dot(normed[i, :, j * depth : (j + 1) * depth], wb[j].reshape(depth, width))
        da_q = pair_norm(acc[:, 0:wide], gains_ref[0:1, :]).astype(BF16)
        da_k = pair_norm(acc[:, wide : 2 * wide], gains_ref[1:2, :]).astype(BF16)
        da_v = acc[:, 2 * wide : 3 * wide].astype(BF16)
        sw_q = pair_norm(acc[:, 3 * wide : 4 * wide], gains_ref[2:3, :]).astype(BF16)
        sw_kv = acc[:, 4 * wide : 5 * wide]
        lane = lax.broadcasted_iota(jnp.int32, sw_kv.shape, 1)
        sw_kv = jnp.where(lane < HD, pair_norm(sw_kv, gains_ref[3:4, :]), sw_kv).astype(BF16)
        scale = jnp.asarray(HD ** (-0.5), BF16)
        query[i, :, 0:wide] = da_q * scale
        query[i, :, wide : 2 * wide] = sw_q * scale
        kv[c, i, :, 0:wide] = da_k
        kv[c, i, :, wide : 2 * wide] = da_v
        kv[c, i, :, 2 * wide : 3 * wide] = sw_kv

    swap = remote(kv.at[c], kv.at[c], kv_send, kv_recv, peer)
    go(swap)
    remote(scal.at[1 - c], scal.at[1 - c], sc_send, sc_recv, peer).wait_recv()
    remote(kv.at[1 - c], kv.at[1 - c], kv_send, kv_recv, peer).wait_recv()

    mine = scal[z // CORES, z % CORES]
    mix = mine[0:1, :]
    def send_rows(i, j):
        cols = pl.ds(j * wide, wide)
        away = (z != i) | jnp.logical_not(owner)
        go(
            remote(
                rows_out.at[i, :, cols],
                rows_in.at[z % CORES, c, :, cols],
                r_send.at[i, j],
                r_recv.at[z % CORES, c, j],
                at(i, z // CORES),
            ),
            away,
        )

    for i in range(n):
        before = jnp.maximum(i - 1 + c, 0)
        q_row = lax.broadcasted_iota(jnp.int32, (tile, tile), 0)
        k_row = lax.broadcasted_iota(jnp.int32, (tile, tile), 1)
        first_ok = (2 * i + c) > 0
        near = kv[c, i, :, 2 * wide : 3 * wide]
        far = kv[1 - c, before, :, 2 * wide : 3 * wide]
        results = []
        for g in range(2):
            q = query[i, :, wide + g * HD : wide + (g + 1) * HD]
            s_near = jnp.where(k_row <= q_row, dot_t(q, near[:, 0:HD]), -jnp.inf)
            s_far = jnp.where((k_row > q_row) & first_ok, dot_t(q, far[:, 0:HD]), -jnp.inf)
            sink = mine[1 + g : 2 + g, 0:1]
            top = jnp.maximum(
                jnp.max(s_near, axis=-1, keepdims=True), jnp.max(s_far, axis=-1, keepdims=True)
            )
            top = jnp.maximum(top, sink)
            w_near = jnp.exp(s_near - top)
            w_far = jnp.exp(s_far - top)
            total = (
                jnp.sum(w_near, axis=-1, keepdims=True)
                + jnp.sum(w_far, axis=-1, keepdims=True)
                + jnp.exp(sink - top)
            )
            summed = dot(w_near.astype(BF16), near[:, HD:wide]) + dot(
                w_far.astype(BF16), far[:, HD:wide]
            )
            results.append(summed / total)
        rows_out[i, :, wide : 2 * wide] = jnp.concatenate(results, axis=-1).astype(BF16)

        send_rows(i, 1)

    for i in range(n):
        q_place = (2 * i + c) * tile + lax.broadcasted_iota(jnp.int32, (tile, 1), 0)
        count = (i + 1) * tile
        column = lax.broadcasted_iota(jnp.int32, (1, count), 1)
        maps = []
        for m in range(2):
            q = query[i, :, m * HD : (m + 1) * HD]
            scores = []
            for h in range(2):
                keys = kv[h, 0 : i + 1, :, m * HD : (m + 1) * HD].reshape(count, HD)
                place = (column // tile) * (2 * tile) + h * tile + column % tile
                scores.append(jnp.where(place <= q_place, dot_t(q, keys), -jnp.inf))
            top = jnp.maximum(
                jnp.max(scores[0], axis=-1, keepdims=True),
                jnp.max(scores[1], axis=-1, keepdims=True),
            )
            total = 0.0
            summed = 0.0
            for h in range(2):
                weights = jnp.exp(scores[h] - top)
                total += jnp.sum(weights, axis=-1, keepdims=True)
                values = kv[h, 0 : i + 1, :, wide : 2 * wide].reshape(count, wide)
                summed += dot(weights.astype(BF16), values)
            maps.append(summed / total)
        blend = maps[0] - mix * maps[1]
        rows_out[i, :, 0:wide] = rms_norm(blend, gains_ref[4:5, :]).astype(BF16)

        send_rows(i, 0)

    keep_rows = pltpu.make_async_copy(rows_out.at[z], rows_in.at[z % CORES, c], local_sem.at[3])
    pl.when(owner)(keep_rows.start)
    pl.when(owner)(keep_rows.wait)

    def await_rows(cc):
        for par in range(CORES):

            def wait(par=par):
                for j in range(2):
                    cols = pl.ds(j * wide, wide)
                    remote(
                        rows_in.at[par, cc, :, cols],
                        rows_in.at[par, cc, :, cols],
                        r_send.at[0, j],
                        r_recv.at[par, cc, j],
                        peer,
                    ).wait_recv()

            pl.when((CORES * c + par != z) | (cc != c))(wait)

    columns = part_out.shape[1] // 4

    def project(cc, q):
        cols = slice(q * columns, (q + 1) * columns)
        acc = 0.0
        for par in range(CORES):
            rows = rows_in[par, cc]
            acc += dot(rows[:, 0:wide], da_out_ref[par * wide : (par + 1) * wide, cols])
            acc += dot(rows[:, wide : 2 * wide], sw_out_ref[par * wide : (par + 1) * wide, cols])
        return acc.astype(BF16)

    for load in out_loads:
        load.wait()
    await_rows(1 - c)
    for q in range(4):
        part_out[:, q * columns : (q + 1) * columns] = project(1 - c, q)
        cols = pl.ds(q * columns, columns)
        go(remote(part_out.at[:, cols], part_in.at[:, cols], p_send.at[q], p_recv.at[q], peer))
    await_rows(c)
    for q in range(4):
        cols = pl.ds(q * columns, columns)
        mine_part = project(c, q).astype(F32)
        remote(part_out.at[:, cols], part_in.at[:, cols], p_send.at[q], p_recv.at[q], peer).wait_recv()
        both = mine_part + part_in[:, cols].astype(F32)
        sum_out[:, cols] = both.astype(BF16)
        go(remote(sum_out.at[:, cols], sum_in.at[:, cols], s_send.at[q], s_recv.at[q], across))
    for q in range(4):
        cols = pl.ds(q * columns, columns)
        remote(sum_out.at[:, cols], sum_in.at[:, cols], s_send.at[q], s_recv.at[q], across).wait_recv()
        total = sum_out[:, cols].astype(F32) + sum_in[:, cols].astype(F32)
        out_ref[c, :, cols] = total.astype(BF16)
        go(
            remote(
                out_ref.at[c, :, cols], out_ref.at[c, :, cols], o_send.at[q], o_recv.at[q], peer
            )
        )
    for q in range(4):
        cols = pl.ds(q * columns, columns)
        remote(
            out_ref.at[1 - c, :, cols], out_ref.at[1 - c, :, cols], o_send.at[q], o_recv.at[q], peer
        ).wait_recv()
    for copy, when in pending:
        if when is None:
            copy.wait_send()
        else:
            pl.when(when)(copy.wait_send)


def transposed(n, *arrays):
    (
        inputs,
        norm_gain,
        da_query_weight,
        da_key_weight,
        da_value_weight,
        sw_query_weight,
        sw_key_weight,
        sw_value_weight,
        da_query_gain,
        da_key_gain,
        sw_query_gain,
        sw_key_gain,
        mix_lambda,
        head_gain,
        sink_logit,
        da_out_weight,
        sw_out_weight,
    ) = arrays
    rows, d = inputs.shape
    depth = da_query_weight.shape[0]
    wide = 2 * HD
    width = 5 * wide
    piece = depth // 4

    def cut(weight):
        return weight.reshape(2, CORES, piece, weight.shape[1])

    def line(vector):
        return vector.reshape(1, -1)

    pieces = 4
    part = rows // 4
    tile = rows // 2
    DMA = pltpu.SemaphoreType.DMA
    vmem = pl.BlockSpec(memory_space=pltpu.VMEM)
    hbm = pl.BlockSpec(memory_space=pl.ANY)
    out = pl.pallas_call(
        functools.partial(kernel, n),
        out_shape=jax.ShapeDtypeStruct((2, tile, d), BF16),
        in_specs=[hbm] * 5 + [vmem] * 10 + [hbm] * 2,
        out_specs=vmem,
        scratch_shapes=[
            pltpu.VMEM(da_out_weight.shape, BF16),
            pltpu.VMEM(sw_out_weight.shape, BF16),
            pltpu.VMEM((CORES, 2, CORES, piece, wide), BF16),
            pltpu.VMEM((8, wide), F32),
            pltpu.VMEM((n, 2, pieces, part // pieces, d), BF16),
            pltpu.VMEM((n, 2, CORES, piece, width), BF16),
            pltpu.VMEM((n, tile, d), BF16),
            pltpu.VMEM((n, tile, 2 * wide), BF16),
            pltpu.VMEM((2, n, tile, 3 * wide), BF16),
            pltpu.VMEM((CORES, CORES, 8, wide), F32),
            pltpu.VMEM((n, tile, 2 * wide), BF16),
            pltpu.VMEM((CORES, CORES, tile, 2 * wide), BF16),
            pltpu.VMEM((tile, d), BF16),
            pltpu.VMEM((tile, d), BF16),
            pltpu.VMEM((tile, d), BF16),
            pltpu.VMEM((tile, d), BF16),
            DMA((6,)),
            DMA((2, n, pieces)),
            DMA((2, n, pieces)),
            DMA((n, pieces)),
            DMA((n, pieces)),
            DMA((CORES, CORES)),
            DMA((n,)),
            DMA((n,)),
            DMA((n,)),
            DMA((2, n)),
            DMA((2, n)),
            DMA,
            DMA,
            DMA,
            DMA,
            DMA,
            DMA,
            DMA((n, 2)),
            DMA((CORES, CORES, 2)),
            DMA((4,)),
            DMA((4,)),
            DMA((4,)),
            DMA((4,)),
            DMA((4,)),
            DMA((4,)),
        ],
        compiler_params=pltpu.CompilerParams(
            collective_id=0, has_side_effects=True, vmem_limit_bytes=60 * 1024 * 1024
        ),
    )(
        inputs.reshape(CORES, 2, pieces, part // pieces, d),
        cut(da_query_weight),
        cut(da_key_weight),
        cut(da_value_weight),
        cut(sw_query_weight),
        cut(sw_key_weight),
        cut(sw_value_weight),
        line(norm_gain),
        line(da_query_gain),
        line(da_key_gain),
        line(sw_query_gain),
        line(sw_key_gain),
        line(head_gain),
        line(mix_lambda),
        line(sink_logit),
        da_out_weight,
        sw_out_weight,
    )
    return out.reshape(rows, d)


def body(sizes, *arrays):
    rows = arrays[0].shape[0]
    heads = arrays[12].shape[0]
    sinks = arrays[14].shape[0]
    n = sizes["sp"]
    fits = (
        sizes["grp"] == 2
        and sizes["tp"] == 2 * CORES
        and n == 2 * CORES
        and heads == CORES
        and sinks == 2 * CORES
        and arrays[6].shape[1] == CORES * HD
        and rows == 2 * WINDOW
    )
    if fits:
        return transposed(n, *arrays)
    return on_device(*arrays)


def solution(mesh):
    return jax.shard_map(
        functools.partial(body, dict(mesh.shape)),
        mesh=mesh,
        in_specs=(
            P(("grp", "sp"), None),
            P(),
            P("sp", "tp"),
            P("sp", "tp"),
            P("sp", "tp"),
            P("sp", "tp"),
            P("sp", "tp"),
            P("sp", "tp"),
            P(),
            P(),
            P(),
            P(),
            P("tp"),
            P(),
            P("tp"),
            P("tp", None),
            P("tp", None),
        ),
        out_specs=P(("grp", "sp"), None),
        check_vma=False,
    )
```

```python
import functools

import jax
import jax.numpy as jnp
from jax import lax
from jax.experimental import pallas as pl
from jax.experimental.pallas import tpu as pltpu
from jax.sharding import PartitionSpec as P

HD = 64
WINDOW = 128


def shifted(value, axis, steps):
    count = lax.axis_size(axis)
    first, last = (max(0, -steps), min(count, count - steps))
    return lax.ppermute(value, axis, [(source, source + steps) for source in range(first, last)])


def rms_norm(values, gain):
    return values * lax.rsqrt(jnp.mean(values * values, axis=-1, keepdims=True) + 1e-06) * gain


def absorb(state, queries, places, keys, values, key_places):
    top, total, summed = state
    scores = jnp.einsum(
        "qhmd,khmd->hmqk", queries, keys, preferred_element_type=jnp.float32
    ) * HD ** (-0.5)
    scores = jnp.where(key_places[None, :] <= places[:, None], scores, -jnp.inf)
    new_top = jnp.maximum(top, jnp.max(scores, axis=-1))
    weights = jnp.exp(scores - new_top[..., None])
    total = jnp.sum(weights, axis=-1)
    summed = jnp.einsum(
        "hmqk,khe->hmqe", weights.astype(jnp.bfloat16), values, preferred_element_type=jnp.float32
    )
    return (new_top, total, summed)


def keep(state, queries, places, keys, values, key_places):
    return state


def diff_attention(queries, places, da_key, da_value, mix_lambda, head_gain):
    rows = queries.shape[0]
    heads = queries.shape[1]
    half = rows // 2
    fresh = (
        jnp.full((heads, 2, half), -1e30, jnp.float32),
        jnp.zeros((heads, 2, half), jnp.float32),
        jnp.zeros((heads, 2, half, 2 * HD), jnp.float32),
    )
    states = (fresh, fresh)
    start = jnp.int32(0)
    keys = lax.all_gather(da_key, "sp", axis=0, tiled=True)
    values = lax.all_gather(da_value, "sp", axis=0, tiled=True)
    key_places = jnp.arange(keys.shape[0], dtype=jnp.int32)
    updated = []
    for section in range(2):
        own_rows = queries[section * half : (section + 1) * half]
        own_places = places[section * half : (section + 1) * half]
        updated.append(
            lax.cond(
                start <= jnp.max(own_places),
                absorb,
                keep,
                states[section],
                own_rows,
                own_places,
                keys,
                values,
                key_places,
            )
        )
    states = tuple(updated)
    blended = []
    for top, total, summed in states:
        maps = summed / total[..., None]
        blended.append(maps[:, 0] - mix_lambda[:, None, None] * maps[:, 1])
    blend = jnp.transpose(jnp.concatenate(blended, axis=1), (1, 0, 2))
    return rms_norm(blend, head_gain).astype(jnp.bfloat16).reshape(rows, heads * 2 * HD)


def window_attention(sw_query, sw_key, sw_value, earlier_key, earlier_value, sink_logit, first):
    rows = sw_query.shape[0]
    sw_heads = sw_query.shape[1]
    kv_heads = sw_key.shape[1]
    groups = sw_heads // kv_heads
    count = rows // WINDOW

    def band(own, earlier_tile):
        tiles = own.reshape(count, WINDOW, kv_heads, HD)
        earlier = jnp.concatenate([earlier_tile[None], tiles[:-1]], axis=0)
        return jnp.concatenate([earlier, tiles], axis=1)

    key_band = band(sw_key, earlier_key)
    value_band = band(sw_value, earlier_value)
    query_tiles = sw_query.reshape(count, WINDOW, kv_heads, groups, HD)
    scores = jnp.einsum(
        "nqhgd,nkhd->nhgqk", query_tiles, key_band, preferred_element_type=jnp.float32
    ) * HD ** (-0.5)
    lag = WINDOW + jnp.arange(WINDOW)[:, None] - jnp.arange(2 * WINDOW)[None, :]
    key_places = (
        first + jnp.arange(count)[:, None] * WINDOW - WINDOW + jnp.arange(2 * WINDOW)[None, :]
    )
    valid = ((lag >= 0) & (lag < WINDOW))[None] & (key_places >= 0)[:, None, :]
    scores = jnp.where(valid[:, None, None], scores, -jnp.inf)
    sink = sink_logit.reshape(kv_heads, groups)[None, :, :, None]
    top = jnp.maximum(jnp.max(scores, axis=-1), sink)
    weights = jnp.exp(scores - top[..., None])
    total = jnp.sum(weights, axis=-1) + jnp.exp(sink - top)
    summed = jnp.einsum(
        "nhgqk,nkhd->nqhgd",
        weights.astype(jnp.bfloat16),
        value_band,
        preferred_element_type=jnp.float32,
    )
    return (
        (summed / jnp.transpose(total, (0, 3, 1, 2))[..., None])
        .astype(jnp.bfloat16)
        .reshape(rows, sw_heads * HD)
    )


def on_device(
    inputs,
    norm_gain,
    da_query_weight,
    da_key_weight,
    da_value_weight,
    sw_query_weight,
    sw_key_weight,
    sw_value_weight,
    da_query_gain,
    da_key_gain,
    sw_query_gain,
    sw_key_gain,
    mix_lambda,
    head_gain,
    sink_logit,
    da_out_weight,
    sw_out_weight,
):
    rows = inputs.shape[0]
    normed = rms_norm(inputs.astype(jnp.float32), norm_gain).astype(jnp.bfloat16)
    pieces = (
        lax.all_gather(da_query_weight, "sp", axis=0, tiled=True),
        lax.all_gather(da_key_weight, "sp", axis=0, tiled=True),
        lax.all_gather(da_value_weight, "sp", axis=0, tiled=True),
        lax.all_gather(sw_query_weight, "sp", axis=0, tiled=True),
        lax.all_gather(sw_key_weight, "sp", axis=0, tiled=True),
        lax.all_gather(sw_value_weight, "sp", axis=0, tiled=True),
    )
    projected = tuple(
        (jnp.dot(normed, piece, preferred_element_type=jnp.float32) for piece in pieces)
    )
    da_heads = da_query_weight.shape[1] // (2 * HD)
    sw_heads = sw_query_weight.shape[1] // HD
    kv_heads = sw_key_weight.shape[1] // HD
    da_query = rms_norm(projected[0].reshape(rows, da_heads, 2, HD), da_query_gain).astype(
        jnp.bfloat16
    )
    da_key = rms_norm(projected[1].reshape(rows, da_heads, 2, HD), da_key_gain).astype(jnp.bfloat16)
    da_value = projected[2].astype(jnp.bfloat16).reshape(rows, da_heads, 2 * HD)
    sw_query = rms_norm(projected[3].reshape(rows, sw_heads, HD), sw_query_gain).astype(
        jnp.bfloat16
    )
    sw_key = rms_norm(projected[4].reshape(rows, kv_heads, HD), sw_key_gain).astype(jnp.bfloat16)
    sw_value = projected[5].astype(jnp.bfloat16).reshape(rows, kv_heads, HD)
    place = lax.axis_index("sp")
    first = place * rows
    earlier_key, earlier_value = shifted(
        (sw_key[rows - WINDOW :], sw_value[rows - WINDOW :]), "sp", 1
    )
    sw_rows = window_attention(
        sw_query, sw_key, sw_value, earlier_key, earlier_value, sink_logit, first
    )
    places = first + jnp.arange(rows, dtype=jnp.int32)
    da_rows = diff_attention(da_query, places, da_key, da_value, mix_lambda, head_gain)
    partial_value = jnp.dot(da_rows, da_out_weight, preferred_element_type=jnp.float32) + jnp.dot(
        sw_rows, sw_out_weight, preferred_element_type=jnp.float32
    )
    return lax.psum(partial_value.astype(jnp.bfloat16), "tp")


MESH = pl.DeviceIdType.MESH
F32, BF16 = jnp.float32, jnp.bfloat16
CORES = 2


def dot(a, b):
    return jnp.dot(a, b, preferred_element_type=F32)


def dot_t(a, b):
    return lax.dot_general(a, b, (((1,), (1,)), ((), ())), preferred_element_type=F32)


def pair_norm(values, gain):
    lane = lax.broadcasted_iota(jnp.int32, values.shape, 1)
    squares = values * values
    low = jnp.sum(jnp.where(lane < HD, squares, 0.0), axis=-1, keepdims=True)
    high = jnp.sum(jnp.where(lane < HD, 0.0, squares), axis=-1, keepdims=True)
    mean = jnp.where(lane < HD, low, high) * (1.0 / HD)
    return values * lax.rsqrt(mean + 1e-06) * gain


def kernel(
    n,
    x_ref,
    da_q_ref,
    da_k_ref,
    da_v_ref,
    sw_q_ref,
    sw_k_ref,
    sw_v_ref,
    norm_gain_ref,
    da_q_gain_ref,
    da_k_gain_ref,
    sw_q_gain_ref,
    sw_k_gain_ref,
    head_gain_ref,
    mix_ref,
    sink_ref,
    da_out_hbm,
    sw_out_hbm,
    out_ref,
    da_out_ref,
    sw_out_ref,
    wp,
    gains_ref,
    xg,
    wb,
    normed,
    query,
    kv,
    scal,
    rows_out,
    rows_in,
    part_out,
    part_in,
    sum_out,
    sum_in,
    local_sem,
    x_send,
    x_recv,
    xf_send,
    xf_recv,
    w_send,
    w_recv,
    wy_send,
    wy_recv,
    wc_send,
    wc_recv,
    own_send,
    own_recv,
    kv_send,
    kv_recv,
    sc_send,
    sc_recv,
    r_send,
    r_recv,
    p_send,
    p_recv,
    s_send,
    s_recv,
    o_send,
    o_recv,
):
    y = lax.axis_index("grp")
    z = lax.axis_index("sp")
    t = lax.axis_index("tp")
    x = t // CORES
    c = t % CORES
    peer = {"tp": x * CORES + 1 - c}
    across = {"tp": (1 - x) * CORES + c}
    beside = {"grp": 1 - y}

    def at(zz, cc):
        return {"sp": zz, "tp": x * CORES + cc}

    def remote(src, dst, send, recv, device):
        return pltpu.make_async_remote_copy(
            src_ref=src,
            dst_ref=dst,
            send_sem=send,
            recv_sem=recv,
            device_id=device,
            device_id_type=MESH,
        )

    barrier = pltpu.get_barrier_semaphore()

    def greet(device):
        pl.semaphore_signal(barrier, inc=1, device_id=device, device_id_type=MESH)

    greet(peer)
    greet(across)
    greet(beside)
    for k in range(1, n):
        for cc in range(CORES):
            greet(at(lax.rem(z + k, n), cc))

    own_x = pltpu.make_async_copy(x_ref.at[c], xg.at[z], local_sem.at[1])
    own_x.start()
    out_loads = [
        pltpu.make_async_copy(da_out_hbm, da_out_ref, local_sem.at[4]),
        pltpu.make_async_copy(sw_out_hbm, sw_out_ref, local_sem.at[5]),
    ]
    for load in out_loads:
        load.start()

    wide = 2 * HD
    packs = []
    for par in range(CORES):
        for j, ref in enumerate((da_q_ref, da_k_ref, da_v_ref, sw_q_ref)):
            packs.append(
                pltpu.make_async_copy(
                    ref.at[:, :, :, :, pl.ds(par * wide, wide)],
                    wp.at[par, :, :, :, :, pl.ds(j * wide, wide)],
                    local_sem.at[6 + par * 4 + j],
                )
            )
    for pack in packs:
        pack.start()

    for par in range(CORES):
        cols = slice(par * HD, (par + 1) * HD)
        wp[par, :, :, :, :, 4 * wide : 5 * wide] = jnp.concatenate([sw_k_ref[..., cols], sw_v_ref[..., cols]], axis=-1)
        scal[c, par, 0:1, :] = jnp.broadcast_to(mix_ref[:, par : par + 1], (1, wide))
        for g in range(2):
            sink = sink_ref[:, 2 * par + g : 2 * par + g + 1]
            scal[c, par, 1 + g : 2 + g, :] = jnp.broadcast_to(sink, (1, wide))
    for i, ref in enumerate((da_q_gain_ref, da_k_gain_ref, sw_q_gain_ref, sw_k_gain_ref)):
        gains_ref[i : i + 1, :] = jnp.concatenate([ref[...], ref[...]], axis=-1)
    gains_ref[4:5, :] = head_gain_ref[...]
    pl.semaphore_wait(barrier, 3 + (n - 1) * CORES)

    pending = []

    def go(copy, when=None):
        if when is None:
            copy.start()
        else:
            pl.when(when)(copy.start)
        pending.append((copy, when))

    pieces = xg.shape[2]

    def hop(d, k, p):
        source = z - k if d == 0 else z + k
        source = jnp.clip(source, 0, n - 1)
        target = jnp.clip(z + 1 if d == 0 else z - 1, 0, n - 1)
        src = xg.at[source, x, p]
        return remote(
            src, xg.at[source, x, p], x_send.at[d, k, p], x_recv.at[d, k, p], {"sp": target}
        )

    def can_hop(d, k):
        return (z - k >= 0) & (z + 1 < n) if d == 0 else (z + k < n) & (z >= 1)

    def has(d, k):
        return z - k >= 0 if d == 0 else z + k < n

    def from_there(d, k):
        return jnp.clip(z - k if d == 0 else z + k, 0, n - 1)

    own_x.wait()
    for p in range(pieces):
        for d in range(2):
            go(hop(d, 0, p), can_hop(d, 0))

    owner = c == z // CORES

    for pack in packs:
        pack.wait()
    own = remote(wp.at[z % CORES], wb.at[z], own_send, own_recv, peer)
    own_local = pltpu.make_async_copy(wp.at[z % CORES], wb.at[z], local_sem.at[0])

    sc = remote(scal.at[c], scal.at[c], sc_send, sc_recv, peer)
    go(sc)

    def cross(zs, p):
        return remote(
            xg.at[zs, x, p], xg.at[zs, x, p], xf_send.at[zs, p], xf_recv.at[zs, p], across
        )

    def weight_direct(zs, s):
        return remote(
            wb.at[zs, y, c, s], wb.at[zs, y, c, s], w_send.at[0, 0, s], w_recv.at[zs, s], peer
        )

    def weight_beside(zs, yy, s):
        return remote(
            wb.at[zs, yy, c, s], wb.at[zs, yy, c, s], wy_send.at[zs, s], wy_recv.at[zs, s], beside
        )

    def weight_core(zs, which, cc, s):
        ref = wb.at[zs, y if which == 0 else 1 - y, cc, s]
        return remote(ref, ref, wc_send.at[which, zs, s], wc_recv.at[which, zs, s], peer)

    def pass_on(k, p):
        for d in range(2):
            zs = from_there(d, k)

            def arrived(zs=zs, d=d):
                remote(
                    xg.at[zs, x, p],
                    xg.at[zs, x, p],
                    x_send.at[d, k - 1, p],
                    x_recv.at[d, k - 1, p],
                    across,
                ).wait_recv()

            pl.when(has(d, k))(arrived)
            if k < n - 1:
                go(hop(d, k, p), can_hop(d, k))
            go(cross(zs, p), has(d, k))

    def send_weights(s):
        for par in range(CORES):
            zt = CORES * c + par
            for cd in range(CORES):
                go(
                    remote(
                        wp.at[par, y, cd, s],
                        wb.at[z, y, cd, s],
                        w_send.at[par, cd, s],
                        w_recv.at[z, s],
                        at(zt, cd),
                    ),
                    zt != z,
                )

    def pass_weights(k, s):
        for d in range(2):
            zs = from_there(d, k)
            pl.when(has(d, k))(lambda zs=zs: weight_direct(zs, s).wait_recv())
            go(weight_beside(zs, y, s), has(d, k))
            go(weight_core(zs, 0, c, s), has(d, k))

    def pass_beside(k, s):
        for d in range(2):
            zs = from_there(d, k)
            pl.when(has(d, k))(lambda zs=zs: weight_beside(zs, 1 - y, s).wait_recv())
            go(weight_core(zs, 1, c, s), has(d, k))

    part = xg.shape[2] * xg.shape[3]
    tile = 2 * part

    def norm_of(i):
        for h in range(2):
            values = xg[i, h].reshape(part, xg.shape[4]).astype(F32)
            values = rms_norm(values, norm_gain_ref[...])
            normed[i, h * part : (h + 1) * part, :] = values.astype(BF16)

    others = [lax.rem(z + k, n) for k in range(1, n)]
    pl.when(owner)(own_local.start)
    go(own, owner)
    for p in range(pieces):
        send_weights(p)
    for p in range(pieces):
        pass_on(1, p)
    for p in range(pieces):
        for k in range(1, n):
            pass_weights(k, p)
        if p:
            pass_on(2, p - 1)
    pass_on(2, pieces - 1)
    norm_of(z)
    for p in range(pieces):
        pass_on(3, p)
    for p in range(pieces):
        for k in range(1, n):
            pass_beside(k, p)

    for k in range(1, n):
        for d in range(2):

            @pl.when(has(d, k))
            def _(zs=from_there(d, k)):
                for p in range(pieces):
                    remote(
                        xg.at[zs, 1 - x, p],
                        xg.at[zs, 1 - x, p],
                        xf_send.at[zs, p],
                        xf_recv.at[zs, p],
                        across,
                    ).wait_recv()
                norm_of(zs)

    pl.when(owner)(own_local.wait)
    pl.when(jnp.logical_not(owner))(own.wait_recv)
    for zs in others:
        for which in range(2):
            for p in range(pieces):
                weight_core(zs, which, 1 - c, p).wait_recv()

    depth = wb.shape[1] * wb.shape[2] * wb.shape[3] * wb.shape[4]
    width = wb.shape[5]
    for i in range(n):
        acc = dot(normed[i, :, 0:depth], wb[0].reshape(depth, width))
        for j in range(1, n):
            acc += dot(normed[i, :, j * depth : (j + 1) * depth], wb[j].reshape(depth, width))
        da_q = pair_norm(acc[:, 0:wide], gains_ref[0:1, :]).astype(BF16)
        da_k = pair_norm(acc[:, wide : 2 * wide], gains_ref[1:2, :]).astype(BF16)
        da_v = acc[:, 2 * wide : 3 * wide].astype(BF16)
        sw_q = pair_norm(acc[:, 3 * wide : 4 * wide], gains_ref[2:3, :]).astype(BF16)
        sw_kv = acc[:, 4 * wide : 5 * wide]
        lane = lax.broadcasted_iota(jnp.int32, sw_kv.shape, 1)
        sw_kv = jnp.where(lane < HD, pair_norm(sw_kv, gains_ref[3:4, :]), sw_kv).astype(BF16)
        scale = jnp.asarray(HD ** (-0.5), BF16)
        query[i, :, 0:wide] = da_q * scale
        query[i, :, wide : 2 * wide] = sw_q * scale
        kv[c, i, :, 0:wide] = da_k
        kv[c, i, :, wide : 2 * wide] = da_v
        kv[c, i, :, 2 * wide : 3 * wide] = sw_kv

    swap = remote(kv.at[c], kv.at[c], kv_send, kv_recv, peer)
    go(swap)
    remote(scal.at[1 - c], scal.at[1 - c], sc_send, sc_recv, peer).wait_recv()
    remote(kv.at[1 - c], kv.at[1 - c], kv_send, kv_recv, peer).wait_recv()

    mine = scal[z // CORES, z % CORES]
    mix = mine[0:1, :]
    def send_rows(i, j):
        cols = pl.ds(j * wide, wide)
        away = (z != i) | jnp.logical_not(owner)
        go(
            remote(
                rows_out.at[i, :, cols],
                rows_in.at[z % CORES, c, :, cols],
                r_send.at[i, j],
                r_recv.at[z % CORES, c, j],
                at(i, z // CORES),
            ),
            away,
        )

    for i in range(n):
        before = jnp.maximum(i - 1 + c, 0)
        q_row = lax.broadcasted_iota(jnp.int32, (tile, tile), 0)
        k_row = lax.broadcasted_iota(jnp.int32, (tile, tile), 1)
        first_ok = (2 * i + c) > 0
        near = kv[c, i, :, 2 * wide : 3 * wide]
        far = kv[1 - c, before, :, 2 * wide : 3 * wide]
        results = []
        for g in range(2):
            q = query[i, :, wide + g * HD : wide + (g + 1) * HD]
            s_near = jnp.where(k_row <= q_row, dot_t(q, near[:, 0:HD]), -jnp.inf)
            s_far = jnp.where((k_row > q_row) & first_ok, dot_t(q, far[:, 0:HD]), -jnp.inf)
            sink = mine[1 + g : 2 + g, 0:1]
            top = jnp.maximum(
                jnp.max(s_near, axis=-1, keepdims=True), jnp.max(s_far, axis=-1, keepdims=True)
            )
            top = jnp.maximum(top, sink)
            w_near = jnp.exp(s_near - top)
            w_far = jnp.exp(s_far - top)
            total = (
                jnp.sum(w_near, axis=-1, keepdims=True)
                + jnp.sum(w_far, axis=-1, keepdims=True)
                + jnp.exp(sink - top)
            )
            summed = dot(w_near.astype(BF16), near[:, HD:wide]) + dot(
                w_far.astype(BF16), far[:, HD:wide]
            )
            results.append(summed / total)
        rows_out[i, :, wide : 2 * wide] = jnp.concatenate(results, axis=-1).astype(BF16)

        send_rows(i, 1)

    for i in range(n):
        q_place = (2 * i + c) * tile + lax.broadcasted_iota(jnp.int32, (tile, 1), 0)
        count = (i + 1) * tile
        column = lax.broadcasted_iota(jnp.int32, (1, count), 1)
        maps = []
        for m in range(2):
            q = query[i, :, m * HD : (m + 1) * HD]
            scores = []
            for h in range(2):
                keys = kv[h, 0 : i + 1, :, m * HD : (m + 1) * HD].reshape(count, HD)
                place = (column // tile) * (2 * tile) + h * tile + column % tile
                scores.append(jnp.where(place <= q_place, dot_t(q, keys), -jnp.inf))
            top = jnp.maximum(
                jnp.max(scores[0], axis=-1, keepdims=True),
                jnp.max(scores[1], axis=-1, keepdims=True),
            )
            total = 0.0
            summed = 0.0
            for h in range(2):
                weights = jnp.exp(scores[h] - top)
                total += jnp.sum(weights, axis=-1, keepdims=True)
                values = kv[h, 0 : i + 1, :, wide : 2 * wide].reshape(count, wide)
                summed += dot(weights.astype(BF16), values)
            maps.append(summed / total)
        blend = maps[0] - mix * maps[1]
        rows_out[i, :, 0:wide] = rms_norm(blend, gains_ref[4:5, :]).astype(BF16)

        send_rows(i, 0)

    keep_rows = pltpu.make_async_copy(rows_out.at[z], rows_in.at[z % CORES, c], local_sem.at[3])
    pl.when(owner)(keep_rows.start)
    pl.when(owner)(keep_rows.wait)

    def await_rows(cc):
        for par in range(CORES):

            def wait(par=par):
                for j in range(2):
                    cols = pl.ds(j * wide, wide)
                    remote(
                        rows_in.at[par, cc, :, cols],
                        rows_in.at[par, cc, :, cols],
                        r_send.at[0, j],
                        r_recv.at[par, cc, j],
                        peer,
                    ).wait_recv()

            pl.when((CORES * c + par != z) | (cc != c))(wait)

    columns = part_out.shape[1] // 4

    def project(cc, q):
        cols = slice(q * columns, (q + 1) * columns)
        acc = 0.0
        for par in range(CORES):
            rows = rows_in[par, cc]
            acc += dot(rows[:, 0:wide], da_out_ref[par * wide : (par + 1) * wide, cols])
            acc += dot(rows[:, wide : 2 * wide], sw_out_ref[par * wide : (par + 1) * wide, cols])
        return acc.astype(BF16)

    for load in out_loads:
        load.wait()
    await_rows(1 - c)
    for q in range(4):
        part_out[:, q * columns : (q + 1) * columns] = project(1 - c, q)
        cols = pl.ds(q * columns, columns)
        go(remote(part_out.at[:, cols], part_in.at[:, cols], p_send.at[q], p_recv.at[q], peer))
    await_rows(c)
    for q in range(4):
        cols = pl.ds(q * columns, columns)
        mine_part = project(c, q).astype(F32)
        remote(part_out.at[:, cols], part_in.at[:, cols], p_send.at[q], p_recv.at[q], peer).wait_recv()
        both = mine_part + part_in[:, cols].astype(F32)
        sum_out[:, cols] = both.astype(BF16)
        go(remote(sum_out.at[:, cols], sum_in.at[:, cols], s_send.at[q], s_recv.at[q], across))
    for q in range(4):
        cols = pl.ds(q * columns, columns)
        remote(sum_out.at[:, cols], sum_in.at[:, cols], s_send.at[q], s_recv.at[q], across).wait_recv()
        total = sum_out[:, cols].astype(F32) + sum_in[:, cols].astype(F32)
        out_ref[c, :, cols] = total.astype(BF16)
        go(
            remote(
                out_ref.at[c, :, cols], out_ref.at[c, :, cols], o_send.at[q], o_recv.at[q], peer
            )
        )
    for q in range(4):
        cols = pl.ds(q * columns, columns)
        remote(
            out_ref.at[1 - c, :, cols], out_ref.at[1 - c, :, cols], o_send.at[q], o_recv.at[q], peer
        ).wait_recv()
    for copy, when in pending:
        if when is None:
            copy.wait_send()
        else:
            pl.when(when)(copy.wait_send)


def transposed(n, *arrays):
    (
        inputs,
        norm_gain,
        da_query_weight,
        da_key_weight,
        da_value_weight,
        sw_query_weight,
        sw_key_weight,
        sw_value_weight,
        da_query_gain,
        da_key_gain,
        sw_query_gain,
        sw_key_gain,
        mix_lambda,
        head_gain,
        sink_logit,
        da_out_weight,
        sw_out_weight,
    ) = arrays
    rows, d = inputs.shape
    depth = da_query_weight.shape[0]
    wide = 2 * HD
    width = 5 * wide
    piece = depth // 4

    def cut(weight):
        return weight.reshape(2, CORES, pieces, piece // pieces, weight.shape[1])

    def line(vector):
        return vector.reshape(1, -1)

    pieces = 4
    part = rows // 4
    tile = rows // 2
    DMA = pltpu.SemaphoreType.DMA
    vmem = pl.BlockSpec(memory_space=pltpu.VMEM)
    hbm = pl.BlockSpec(memory_space=pl.ANY)
    out = pl.pallas_call(
        functools.partial(kernel, n),
        out_shape=jax.ShapeDtypeStruct((2, tile, d), BF16),
        in_specs=[hbm] * 5 + [vmem] * 10 + [hbm] * 2,
        out_specs=vmem,
        scratch_shapes=[
            pltpu.VMEM(da_out_weight.shape, BF16),
            pltpu.VMEM(sw_out_weight.shape, BF16),
            pltpu.VMEM((CORES, 2, CORES, pieces, piece // pieces, width), BF16),
            pltpu.VMEM((8, wide), F32),
            pltpu.VMEM((n, 2, pieces, part // pieces, d), BF16),
            pltpu.VMEM((n, 2, CORES, pieces, piece // pieces, width), BF16),
            pltpu.VMEM((n, tile, d), BF16),
            pltpu.VMEM((n, tile, 2 * wide), BF16),
            pltpu.VMEM((2, n, tile, 3 * wide), BF16),
            pltpu.VMEM((CORES, CORES, 8, wide), F32),
            pltpu.VMEM((n, tile, 2 * wide), BF16),
            pltpu.VMEM((CORES, CORES, tile, 2 * wide), BF16),
            pltpu.VMEM((tile, d), BF16),
            pltpu.VMEM((tile, d), BF16),
            pltpu.VMEM((tile, d), BF16),
            pltpu.VMEM((tile, d), BF16),
            DMA((14,)),
            DMA((2, n, pieces)),
            DMA((2, n, pieces)),
            DMA((n, pieces)),
            DMA((n, pieces)),
            DMA((CORES, CORES, pieces)),
            DMA((n, pieces)),
            DMA((n, pieces)),
            DMA((n, pieces)),
            DMA((2, n, pieces)),
            DMA((2, n, pieces)),
            DMA,
            DMA,
            DMA,
            DMA,
            DMA,
            DMA,
            DMA((n, 2)),
            DMA((CORES, CORES, 2)),
            DMA((4,)),
            DMA((4,)),
            DMA((4,)),
            DMA((4,)),
            DMA((4,)),
            DMA((4,)),
        ],
        compiler_params=pltpu.CompilerParams(
            collective_id=0, has_side_effects=True, vmem_limit_bytes=60 * 1024 * 1024
        ),
    )(
        inputs.reshape(CORES, 2, pieces, part // pieces, d),
        cut(da_query_weight),
        cut(da_key_weight),
        cut(da_value_weight),
        cut(sw_query_weight),
        cut(sw_key_weight),
        cut(sw_value_weight),
        line(norm_gain),
        line(da_query_gain),
        line(da_key_gain),
        line(sw_query_gain),
        line(sw_key_gain),
        line(head_gain),
        line(mix_lambda),
        line(sink_logit),
        da_out_weight,
        sw_out_weight,
    )
    return out.reshape(rows, d)


def body(sizes, *arrays):
    rows = arrays[0].shape[0]
    heads = arrays[12].shape[0]
    sinks = arrays[14].shape[0]
    n = sizes["sp"]
    fits = (
        sizes["grp"] == 2
        and sizes["tp"] == 2 * CORES
        and n == 2 * CORES
        and heads == CORES
        and sinks == 2 * CORES
        and arrays[6].shape[1] == CORES * HD
        and rows == 2 * WINDOW
    )
    if fits:
        return transposed(n, *arrays)
    return on_device(*arrays)


def solution(mesh):
    return jax.shard_map(
        functools.partial(body, dict(mesh.shape)),
        mesh=mesh,
        in_specs=(
            P(("grp", "sp"), None),
            P(),
            P("sp", "tp"),
            P("sp", "tp"),
            P("sp", "tp"),
            P("sp", "tp"),
            P("sp", "tp"),
            P("sp", "tp"),
            P(),
            P(),
            P(),
            P(),
            P("tp"),
            P(),
            P("tp"),
            P("tp", None),
            P("tp", None),
        ),
        out_specs=P(("grp", "sp"), None),
        check_vma=False,
    )
```

```python
import functools

import jax
import jax.numpy as jnp
from jax import lax
from jax.experimental import pallas as pl
from jax.experimental.pallas import tpu as pltpu
from jax.sharding import PartitionSpec as P

HD = 64
WINDOW = 128


def shifted(value, axis, steps):
    count = lax.axis_size(axis)
    first, last = (max(0, -steps), min(count, count - steps))
    return lax.ppermute(value, axis, [(source, source + steps) for source in range(first, last)])


def rms_norm(values, gain):
    return values * lax.rsqrt(jnp.mean(values * values, axis=-1, keepdims=True) + 1e-06) * gain


def absorb(state, queries, places, keys, values, key_places):
    top, total, summed = state
    scores = jnp.einsum(
        "qhmd,khmd->hmqk", queries, keys, preferred_element_type=jnp.float32
    ) * HD ** (-0.5)
    scores = jnp.where(key_places[None, :] <= places[:, None], scores, -jnp.inf)
    new_top = jnp.maximum(top, jnp.max(scores, axis=-1))
    weights = jnp.exp(scores - new_top[..., None])
    total = jnp.sum(weights, axis=-1)
    summed = jnp.einsum(
        "hmqk,khe->hmqe", weights.astype(jnp.bfloat16), values, preferred_element_type=jnp.float32
    )
    return (new_top, total, summed)


def keep(state, queries, places, keys, values, key_places):
    return state


def diff_attention(queries, places, da_key, da_value, mix_lambda, head_gain):
    rows = queries.shape[0]
    heads = queries.shape[1]
    half = rows // 2
    fresh = (
        jnp.full((heads, 2, half), -1e30, jnp.float32),
        jnp.zeros((heads, 2, half), jnp.float32),
        jnp.zeros((heads, 2, half, 2 * HD), jnp.float32),
    )
    states = (fresh, fresh)
    start = jnp.int32(0)
    keys = lax.all_gather(da_key, "sp", axis=0, tiled=True)
    values = lax.all_gather(da_value, "sp", axis=0, tiled=True)
    key_places = jnp.arange(keys.shape[0], dtype=jnp.int32)
    updated = []
    for section in range(2):
        own_rows = queries[section * half : (section + 1) * half]
        own_places = places[section * half : (section + 1) * half]
        updated.append(
            lax.cond(
                start <= jnp.max(own_places),
                absorb,
                keep,
                states[section],
                own_rows,
                own_places,
                keys,
                values,
                key_places,
            )
        )
    states = tuple(updated)
    blended = []
    for top, total, summed in states:
        maps = summed / total[..., None]
        blended.append(maps[:, 0] - mix_lambda[:, None, None] * maps[:, 1])
    blend = jnp.transpose(jnp.concatenate(blended, axis=1), (1, 0, 2))
    return rms_norm(blend, head_gain).astype(jnp.bfloat16).reshape(rows, heads * 2 * HD)


def window_attention(sw_query, sw_key, sw_value, earlier_key, earlier_value, sink_logit, first):
    rows = sw_query.shape[0]
    sw_heads = sw_query.shape[1]
    kv_heads = sw_key.shape[1]
    groups = sw_heads // kv_heads
    count = rows // WINDOW

    def band(own, earlier_tile):
        tiles = own.reshape(count, WINDOW, kv_heads, HD)
        earlier = jnp.concatenate([earlier_tile[None], tiles[:-1]], axis=0)
        return jnp.concatenate([earlier, tiles], axis=1)

    key_band = band(sw_key, earlier_key)
    value_band = band(sw_value, earlier_value)
    query_tiles = sw_query.reshape(count, WINDOW, kv_heads, groups, HD)
    scores = jnp.einsum(
        "nqhgd,nkhd->nhgqk", query_tiles, key_band, preferred_element_type=jnp.float32
    ) * HD ** (-0.5)
    lag = WINDOW + jnp.arange(WINDOW)[:, None] - jnp.arange(2 * WINDOW)[None, :]
    key_places = (
        first + jnp.arange(count)[:, None] * WINDOW - WINDOW + jnp.arange(2 * WINDOW)[None, :]
    )
    valid = ((lag >= 0) & (lag < WINDOW))[None] & (key_places >= 0)[:, None, :]
    scores = jnp.where(valid[:, None, None], scores, -jnp.inf)
    sink = sink_logit.reshape(kv_heads, groups)[None, :, :, None]
    top = jnp.maximum(jnp.max(scores, axis=-1), sink)
    weights = jnp.exp(scores - top[..., None])
    total = jnp.sum(weights, axis=-1) + jnp.exp(sink - top)
    summed = jnp.einsum(
        "nhgqk,nkhd->nqhgd",
        weights.astype(jnp.bfloat16),
        value_band,
        preferred_element_type=jnp.float32,
    )
    return (
        (summed / jnp.transpose(total, (0, 3, 1, 2))[..., None])
        .astype(jnp.bfloat16)
        .reshape(rows, sw_heads * HD)
    )


def on_device(
    inputs,
    norm_gain,
    da_query_weight,
    da_key_weight,
    da_value_weight,
    sw_query_weight,
    sw_key_weight,
    sw_value_weight,
    da_query_gain,
    da_key_gain,
    sw_query_gain,
    sw_key_gain,
    mix_lambda,
    head_gain,
    sink_logit,
    da_out_weight,
    sw_out_weight,
):
    rows = inputs.shape[0]
    normed = rms_norm(inputs.astype(jnp.float32), norm_gain).astype(jnp.bfloat16)
    pieces = (
        lax.all_gather(da_query_weight, "sp", axis=0, tiled=True),
        lax.all_gather(da_key_weight, "sp", axis=0, tiled=True),
        lax.all_gather(da_value_weight, "sp", axis=0, tiled=True),
        lax.all_gather(sw_query_weight, "sp", axis=0, tiled=True),
        lax.all_gather(sw_key_weight, "sp", axis=0, tiled=True),
        lax.all_gather(sw_value_weight, "sp", axis=0, tiled=True),
    )
    projected = tuple(
        (jnp.dot(normed, piece, preferred_element_type=jnp.float32) for piece in pieces)
    )
    da_heads = da_query_weight.shape[1] // (2 * HD)
    sw_heads = sw_query_weight.shape[1] // HD
    kv_heads = sw_key_weight.shape[1] // HD
    da_query = rms_norm(projected[0].reshape(rows, da_heads, 2, HD), da_query_gain).astype(
        jnp.bfloat16
    )
    da_key = rms_norm(projected[1].reshape(rows, da_heads, 2, HD), da_key_gain).astype(jnp.bfloat16)
    da_value = projected[2].astype(jnp.bfloat16).reshape(rows, da_heads, 2 * HD)
    sw_query = rms_norm(projected[3].reshape(rows, sw_heads, HD), sw_query_gain).astype(
        jnp.bfloat16
    )
    sw_key = rms_norm(projected[4].reshape(rows, kv_heads, HD), sw_key_gain).astype(jnp.bfloat16)
    sw_value = projected[5].astype(jnp.bfloat16).reshape(rows, kv_heads, HD)
    place = lax.axis_index("sp")
    first = place * rows
    earlier_key, earlier_value = shifted(
        (sw_key[rows - WINDOW :], sw_value[rows - WINDOW :]), "sp", 1
    )
    sw_rows = window_attention(
        sw_query, sw_key, sw_value, earlier_key, earlier_value, sink_logit, first
    )
    places = first + jnp.arange(rows, dtype=jnp.int32)
    da_rows = diff_attention(da_query, places, da_key, da_value, mix_lambda, head_gain)
    partial_value = jnp.dot(da_rows, da_out_weight, preferred_element_type=jnp.float32) + jnp.dot(
        sw_rows, sw_out_weight, preferred_element_type=jnp.float32
    )
    return lax.psum(partial_value.astype(jnp.bfloat16), "tp")


MESH = pl.DeviceIdType.MESH
F32, BF16 = jnp.float32, jnp.bfloat16
CORES = 2


def dot(a, b):
    return jnp.dot(a, b, preferred_element_type=F32)


def dot_t(a, b):
    return lax.dot_general(a, b, (((1,), (1,)), ((), ())), preferred_element_type=F32)


def pair_norm(values, gain):
    lane = lax.broadcasted_iota(jnp.int32, values.shape, 1)
    squares = values * values
    low = jnp.sum(jnp.where(lane < HD, squares, 0.0), axis=-1, keepdims=True)
    high = jnp.sum(jnp.where(lane < HD, 0.0, squares), axis=-1, keepdims=True)
    mean = jnp.where(lane < HD, low, high) * (1.0 / HD)
    return values * lax.rsqrt(mean + 1e-06) * gain


def kernel(
    n,
    x_ref,
    da_q_ref,
    da_k_ref,
    da_v_ref,
    sw_q_ref,
    sw_k_ref,
    sw_v_ref,
    norm_gain_ref,
    da_q_gain_ref,
    da_k_gain_ref,
    sw_q_gain_ref,
    sw_k_gain_ref,
    head_gain_ref,
    mix_ref,
    sink_ref,
    da_out_hbm,
    sw_out_hbm,
    out_ref,
    da_out_ref,
    sw_out_ref,
    wp,
    gains_ref,
    xg,
    wb,
    normed,
    query,
    kv,
    scal,
    rows_out,
    rows_in,
    part_out,
    part_in,
    sum_out,
    sum_in,
    local_sem,
    x_send,
    x_recv,
    xf_send,
    xf_recv,
    w_send,
    w_recv,
    wy_send,
    wy_recv,
    wc_send,
    wc_recv,
    own_send,
    own_recv,
    kv_send,
    kv_recv,
    sc_send,
    sc_recv,
    r_send,
    r_recv,
    p_send,
    p_recv,
    s_send,
    s_recv,
    o_send,
    o_recv,
):
    y = lax.axis_index("grp")
    z = lax.axis_index("sp")
    t = lax.axis_index("tp")
    x = t // CORES
    c = t % CORES
    peer = {"tp": x * CORES + 1 - c}
    across = {"tp": (1 - x) * CORES + c}
    beside = {"grp": 1 - y}

    def at(zz, cc):
        return {"sp": zz, "tp": x * CORES + cc}

    def remote(src, dst, send, recv, device):
        return pltpu.make_async_remote_copy(
            src_ref=src,
            dst_ref=dst,
            send_sem=send,
            recv_sem=recv,
            device_id=device,
            device_id_type=MESH,
        )

    barrier = pltpu.get_barrier_semaphore()

    def greet(device):
        pl.semaphore_signal(barrier, inc=1, device_id=device, device_id_type=MESH)

    greet(peer)
    greet(across)
    greet(beside)
    for k in range(1, n):
        for cc in range(CORES):
            greet(at(lax.rem(z + k, n), cc))

    own_x = pltpu.make_async_copy(x_ref.at[c], xg.at[z], local_sem.at[1])
    own_x.start()
    out_loads = [
        pltpu.make_async_copy(da_out_hbm, da_out_ref, local_sem.at[4]),
        pltpu.make_async_copy(sw_out_hbm, sw_out_ref, local_sem.at[5]),
    ]
    for load in out_loads:
        load.start()

    wide = 2 * HD
    packs = []
    for par in range(CORES):
        for j, ref in enumerate((da_q_ref, da_k_ref, da_v_ref, sw_q_ref)):
            packs.append(
                pltpu.make_async_copy(
                    ref.at[:, :, :, :, pl.ds(par * wide, wide)],
                    wp.at[par, :, :, :, :, pl.ds(j * wide, wide)],
                    local_sem.at[6 + par * 4 + j],
                )
            )
    for pack in packs:
        pack.start()

    for par in range(CORES):
        cols = slice(par * HD, (par + 1) * HD)
        wp[par, :, :, :, :, 4 * wide : 5 * wide] = jnp.concatenate([sw_k_ref[..., cols], sw_v_ref[..., cols]], axis=-1)
        scal[c, par, 0:1, :] = jnp.broadcast_to(mix_ref[:, par : par + 1], (1, wide))
        for g in range(2):
            sink = sink_ref[:, 2 * par + g : 2 * par + g + 1]
            scal[c, par, 1 + g : 2 + g, :] = jnp.broadcast_to(sink, (1, wide))
    for i, ref in enumerate((da_q_gain_ref, da_k_gain_ref, sw_q_gain_ref, sw_k_gain_ref)):
        gains_ref[i : i + 1, :] = jnp.concatenate([ref[...], ref[...]], axis=-1)
    gains_ref[4:5, :] = head_gain_ref[...]
    pl.semaphore_wait(barrier, 3 + (n - 1) * CORES)

    pending = []

    def go(copy, when=None):
        if when is None:
            copy.start()
        else:
            pl.when(when)(copy.start)
        pending.append((copy, when))

    pieces = xg.shape[2]

    def hop(d, k, p):
        source = z - k if d == 0 else z + k
        source = jnp.clip(source, 0, n - 1)
        target = jnp.clip(z + 1 if d == 0 else z - 1, 0, n - 1)
        src = xg.at[source, x, p]
        return remote(
            src, xg.at[source, x, p], x_send.at[d, k, p], x_recv.at[d, k, p], {"sp": target}
        )

    def can_hop(d, k):
        return (z - k >= 0) & (z + 1 < n) if d == 0 else (z + k < n) & (z >= 1)

    def has(d, k):
        return z - k >= 0 if d == 0 else z + k < n

    def from_there(d, k):
        return jnp.clip(z - k if d == 0 else z + k, 0, n - 1)

    own_x.wait()
    for p in range(pieces):
        for d in range(2):
            go(hop(d, 0, p), can_hop(d, 0))

    owner = c == z // CORES

    for pack in packs:
        pack.wait()
    own = remote(wp.at[z % CORES], wb.at[z], own_send, own_recv, peer)
    own_local = pltpu.make_async_copy(wp.at[z % CORES], wb.at[z], local_sem.at[0])

    sc = remote(scal.at[c], scal.at[c], sc_send, sc_recv, peer)
    go(sc)

    def cross(zs, p):
        return remote(
            xg.at[zs, x, p], xg.at[zs, x, p], xf_send.at[zs, p], xf_recv.at[zs, p], across
        )

    def weight_direct(zs, s):
        return remote(
            wb.at[zs, y, c, s], wb.at[zs, y, c, s], w_send.at[0, 0, s], w_recv.at[zs, s], peer
        )

    def weight_beside(zs, yy, s):
        return remote(
            wb.at[zs, yy, c, s], wb.at[zs, yy, c, s], wy_send.at[zs, s], wy_recv.at[zs, s], beside
        )

    def weight_core(zs, which, cc, s):
        ref = wb.at[zs, y if which == 0 else 1 - y, cc, s]
        return remote(ref, ref, wc_send.at[which, zs, s], wc_recv.at[which, zs, s], peer)

    def pass_on(k, p):
        for d in range(2):
            zs = from_there(d, k)

            def arrived(zs=zs, d=d):
                remote(
                    xg.at[zs, x, p],
                    xg.at[zs, x, p],
                    x_send.at[d, k - 1, p],
                    x_recv.at[d, k - 1, p],
                    across,
                ).wait_recv()

            pl.when(has(d, k))(arrived)
            if k < n - 1:
                go(hop(d, k, p), can_hop(d, k))
            go(cross(zs, p), has(d, k))

    def send_weights(s):
        for par in range(CORES):
            zt = CORES * c + par
            for cd in range(CORES):
                go(
                    remote(
                        wp.at[par, y, cd, s],
                        wb.at[z, y, cd, s],
                        w_send.at[par, cd, s],
                        w_recv.at[z, s],
                        at(zt, cd),
                    ),
                    zt != z,
                )

    def pass_weights(k, s):
        for d in range(2):
            zs = from_there(d, k)
            pl.when(has(d, k))(lambda zs=zs: weight_direct(zs, s).wait_recv())
            go(weight_beside(zs, y, s), has(d, k))
            go(weight_core(zs, 0, c, s), has(d, k))

    def pass_beside(k, s):
        for d in range(2):
            zs = from_there(d, k)
            pl.when(has(d, k))(lambda zs=zs: weight_beside(zs, 1 - y, s).wait_recv())
            go(weight_core(zs, 1, c, s), has(d, k))

    part = xg.shape[2] * xg.shape[3]
    tile = 2 * part

    def norm_of(i):
        for h in range(2):
            values = xg[i, h].reshape(part, xg.shape[4]).astype(F32)
            values = rms_norm(values, norm_gain_ref[...])
            normed[i, h * part : (h + 1) * part, :] = values.astype(BF16)

    others = [lax.rem(z + k, n) for k in range(1, n)]
    pl.when(owner)(own_local.start)
    go(own, owner)
    for p in range(pieces):
        send_weights(p)
    for p in range(pieces):
        pass_on(1, p)
    for p in range(pieces):
        for k in range(1, n):
            pass_weights(k, p)
        if p:
            pass_on(2, p - 1)
    pass_on(2, pieces - 1)
    norm_of(z)
    for p in range(pieces):
        pass_on(3, p)
    for p in range(pieces):
        for k in range(1, n):
            pass_beside(k, p)

    for k in range(1, n):
        for d in range(2):

            @pl.when(has(d, k))
            def _(zs=from_there(d, k)):
                for p in range(pieces):
                    remote(
                        xg.at[zs, 1 - x, p],
                        xg.at[zs, 1 - x, p],
                        xf_send.at[zs, p],
                        xf_recv.at[zs, p],
                        across,
                    ).wait_recv()
                norm_of(zs)

    pl.when(owner)(own_local.wait)
    pl.when(jnp.logical_not(owner))(own.wait_recv)
    for zs in others:
        for which in range(2):
            for p in range(pieces):
                weight_core(zs, which, 1 - c, p).wait_recv()

    depth = wb.shape[1] * wb.shape[2] * wb.shape[3] * wb.shape[4]
    width = wb.shape[5]
    for i in range(n):
        acc = dot(normed[i, :, 0:depth], wb[0].reshape(depth, width))
        for j in range(1, n):
            acc += dot(normed[i, :, j * depth : (j + 1) * depth], wb[j].reshape(depth, width))
        da_q = pair_norm(acc[:, 0:wide], gains_ref[0:1, :]).astype(BF16)
        da_k = pair_norm(acc[:, wide : 2 * wide], gains_ref[1:2, :]).astype(BF16)
        da_v = acc[:, 2 * wide : 3 * wide].astype(BF16)
        sw_q = pair_norm(acc[:, 3 * wide : 4 * wide], gains_ref[2:3, :]).astype(BF16)
        sw_kv = acc[:, 4 * wide : 5 * wide]
        lane = lax.broadcasted_iota(jnp.int32, sw_kv.shape, 1)
        sw_kv = jnp.where(lane < HD, pair_norm(sw_kv, gains_ref[3:4, :]), sw_kv).astype(BF16)
        scale = jnp.asarray(HD ** (-0.5), BF16)
        query[i, :, 0:wide] = da_q * scale
        query[i, :, wide : 2 * wide] = sw_q * scale
        kv[c, i, :, 0:wide] = da_k
        kv[c, i, :, wide : 2 * wide] = da_v
        kv[c, i, :, 2 * wide : 3 * wide] = sw_kv

    swap = remote(kv.at[c], kv.at[c], kv_send, kv_recv, peer)
    go(swap)
    remote(scal.at[1 - c], scal.at[1 - c], sc_send, sc_recv, peer).wait_recv()
    remote(kv.at[1 - c], kv.at[1 - c], kv_send, kv_recv, peer).wait_recv()

    mine = scal[z // CORES, z % CORES]
    mix = mine[0:1, :]
    def send_rows(i, j):
        cols = pl.ds(j * wide, wide)
        away = (z != i) | jnp.logical_not(owner)
        go(
            remote(
                rows_out.at[i, :, cols],
                rows_in.at[z % CORES, c, :, cols],
                r_send.at[i, j],
                r_recv.at[z % CORES, c, j],
                at(i, z // CORES),
            ),
            away,
        )

    for i in range(n):
        before = jnp.maximum(i - 1 + c, 0)
        q_row = lax.broadcasted_iota(jnp.int32, (tile, tile), 0)
        k_row = lax.broadcasted_iota(jnp.int32, (tile, tile), 1)
        first_ok = (2 * i + c) > 0
        near = kv[c, i, :, 2 * wide : 3 * wide]
        far = kv[1 - c, before, :, 2 * wide : 3 * wide]
        results = []
        for g in range(2):
            q = query[i, :, wide + g * HD : wide + (g + 1) * HD]
            s_near = jnp.where(k_row <= q_row, dot_t(q, near[:, 0:HD]), -jnp.inf)
            s_far = jnp.where((k_row > q_row) & first_ok, dot_t(q, far[:, 0:HD]), -jnp.inf)
            sink = mine[1 + g : 2 + g, 0:1]
            top = jnp.maximum(
                jnp.max(s_near, axis=-1, keepdims=True), jnp.max(s_far, axis=-1, keepdims=True)
            )
            top = jnp.maximum(top, sink)
            w_near = jnp.exp(s_near - top)
            w_far = jnp.exp(s_far - top)
            total = (
                jnp.sum(w_near, axis=-1, keepdims=True)
                + jnp.sum(w_far, axis=-1, keepdims=True)
                + jnp.exp(sink - top)
            )
            summed = dot(w_near.astype(BF16), near[:, HD:wide]) + dot(
                w_far.astype(BF16), far[:, HD:wide]
            )
            results.append(summed / total)
        rows_out[i, :, wide : 2 * wide] = jnp.concatenate(results, axis=-1).astype(BF16)

        send_rows(i, 1)

    for i in range(n):
        q_place = (2 * i + c) * tile + lax.broadcasted_iota(jnp.int32, (tile, 1), 0)
        count = (i + 1) * tile
        column = lax.broadcasted_iota(jnp.int32, (1, count), 1)
        maps = []
        for m in range(2):
            q = query[i, :, m * HD : (m + 1) * HD]
            scores = []
            for h in range(2):
                keys = kv[h, 0 : i + 1, :, m * HD : (m + 1) * HD].reshape(count, HD)
                place = (column // tile) * (2 * tile) + h * tile + column % tile
                scores.append(jnp.where(place <= q_place, dot_t(q, keys), -jnp.inf))
            top = jnp.maximum(
                jnp.max(scores[0], axis=-1, keepdims=True),
                jnp.max(scores[1], axis=-1, keepdims=True),
            )
            total = 0.0
            summed = 0.0
            for h in range(2):
                weights = jnp.exp(scores[h] - top)
                total += jnp.sum(weights, axis=-1, keepdims=True)
                values = kv[h, 0 : i + 1, :, wide : 2 * wide].reshape(count, wide)
                summed += dot(weights.astype(BF16), values)
            maps.append(summed / total)
        blend = maps[0] - mix * maps[1]
        rows_out[i, :, 0:wide] = rms_norm(blend, gains_ref[4:5, :]).astype(BF16)

        send_rows(i, 0)

    keep_rows = pltpu.make_async_copy(rows_out.at[z], rows_in.at[z % CORES, c], local_sem.at[3])
    pl.when(owner)(keep_rows.start)
    pl.when(owner)(keep_rows.wait)

    def await_rows(cc):
        for par in range(CORES):

            def wait(par=par):
                for j in range(2):
                    cols = pl.ds(j * wide, wide)
                    remote(
                        rows_in.at[par, cc, :, cols],
                        rows_in.at[par, cc, :, cols],
                        r_send.at[0, j],
                        r_recv.at[par, cc, j],
                        peer,
                    ).wait_recv()

            pl.when((CORES * c + par != z) | (cc != c))(wait)

    columns = part_out.shape[1] // 4

    def project(cc, q):
        cols = slice(q * columns, (q + 1) * columns)
        acc = 0.0
        for par in range(CORES):
            rows = rows_in[par, cc]
            acc += dot(rows[:, 0:wide], da_out_ref[par * wide : (par + 1) * wide, cols])
            acc += dot(rows[:, wide : 2 * wide], sw_out_ref[par * wide : (par + 1) * wide, cols])
        return acc.astype(BF16)

    for load in out_loads:
        load.wait()
    await_rows(1 - c)
    for q in range(4 + 1):
        if q < 4:
            part_out[:, q * columns : (q + 1) * columns] = project(1 - c, q)
            cols = pl.ds(q * columns, columns)
            go(remote(part_out.at[:, cols], part_in.at[:, cols], p_send.at[q], p_recv.at[q], peer))
        if q == 0:
            await_rows(c)
            continue
        last = q - 1
        cols = pl.ds(last * columns, columns)
        mine_part = project(c, last).astype(F32)
        remote(
            part_out.at[:, cols], part_in.at[:, cols], p_send.at[last], p_recv.at[last], peer
        ).wait_recv()
        both = mine_part + part_in[:, cols].astype(F32)
        sum_out[:, cols] = both.astype(BF16)
        go(remote(sum_out.at[:, cols], sum_in.at[:, cols], s_send.at[last], s_recv.at[last], across))
    for q in range(4):
        cols = pl.ds(q * columns, columns)
        remote(sum_out.at[:, cols], sum_in.at[:, cols], s_send.at[q], s_recv.at[q], across).wait_recv()
        total = sum_out[:, cols].astype(F32) + sum_in[:, cols].astype(F32)
        out_ref[c, :, cols] = total.astype(BF16)
        go(
            remote(
                out_ref.at[c, :, cols], out_ref.at[c, :, cols], o_send.at[q], o_recv.at[q], peer
            )
        )
    for q in range(4):
        cols = pl.ds(q * columns, columns)
        remote(
            out_ref.at[1 - c, :, cols], out_ref.at[1 - c, :, cols], o_send.at[q], o_recv.at[q], peer
        ).wait_recv()
    for copy, when in pending:
        if when is None:
            copy.wait_send()
        else:
            pl.when(when)(copy.wait_send)


def transposed(n, *arrays):
    (
        inputs,
        norm_gain,
        da_query_weight,
        da_key_weight,
        da_value_weight,
        sw_query_weight,
        sw_key_weight,
        sw_value_weight,
        da_query_gain,
        da_key_gain,
        sw_query_gain,
        sw_key_gain,
        mix_lambda,
        head_gain,
        sink_logit,
        da_out_weight,
        sw_out_weight,
    ) = arrays
    rows, d = inputs.shape
    depth = da_query_weight.shape[0]
    wide = 2 * HD
    width = 5 * wide
    piece = depth // 4

    def cut(weight):
        return weight.reshape(2, CORES, pieces, piece // pieces, weight.shape[1])

    def line(vector):
        return vector.reshape(1, -1)

    pieces = 4
    part = rows // 4
    tile = rows // 2
    DMA = pltpu.SemaphoreType.DMA
    vmem = pl.BlockSpec(memory_space=pltpu.VMEM)
    hbm = pl.BlockSpec(memory_space=pl.ANY)
    out = pl.pallas_call(
        functools.partial(kernel, n),
        out_shape=jax.ShapeDtypeStruct((2, tile, d), BF16),
        in_specs=[hbm] * 5 + [vmem] * 10 + [hbm] * 2,
        out_specs=vmem,
        scratch_shapes=[
            pltpu.VMEM(da_out_weight.shape, BF16),
            pltpu.VMEM(sw_out_weight.shape, BF16),
            pltpu.VMEM((CORES, 2, CORES, pieces, piece // pieces, width), BF16),
            pltpu.VMEM((8, wide), F32),
            pltpu.VMEM((n, 2, pieces, part // pieces, d), BF16),
            pltpu.VMEM((n, 2, CORES, pieces, piece // pieces, width), BF16),
            pltpu.VMEM((n, tile, d), BF16),
            pltpu.VMEM((n, tile, 2 * wide), BF16),
            pltpu.VMEM((2, n, tile, 3 * wide), BF16),
            pltpu.VMEM((CORES, CORES, 8, wide), F32),
            pltpu.VMEM((n, tile, 2 * wide), BF16),
            pltpu.VMEM((CORES, CORES, tile, 2 * wide), BF16),
            pltpu.VMEM((tile, d), BF16),
            pltpu.VMEM((tile, d), BF16),
            pltpu.VMEM((tile, d), BF16),
            pltpu.VMEM((tile, d), BF16),
            DMA((14,)),
            DMA((2, n, pieces)),
            DMA((2, n, pieces)),
            DMA((n, pieces)),
            DMA((n, pieces)),
            DMA((CORES, CORES, pieces)),
            DMA((n, pieces)),
            DMA((n, pieces)),
            DMA((n, pieces)),
            DMA((2, n, pieces)),
            DMA((2, n, pieces)),
            DMA,
            DMA,
            DMA,
            DMA,
            DMA,
            DMA,
            DMA((n, 2)),
            DMA((CORES, CORES, 2)),
            DMA((4,)),
            DMA((4,)),
            DMA((4,)),
            DMA((4,)),
            DMA((4,)),
            DMA((4,)),
        ],
        compiler_params=pltpu.CompilerParams(
            collective_id=0, has_side_effects=True, vmem_limit_bytes=60 * 1024 * 1024
        ),
    )(
        inputs.reshape(CORES, 2, pieces, part // pieces, d),
        cut(da_query_weight),
        cut(da_key_weight),
        cut(da_value_weight),
        cut(sw_query_weight),
        cut(sw_key_weight),
        cut(sw_value_weight),
        line(norm_gain),
        line(da_query_gain),
        line(da_key_gain),
        line(sw_query_gain),
        line(sw_key_gain),
        line(head_gain),
        line(mix_lambda),
        line(sink_logit),
        da_out_weight,
        sw_out_weight,
    )
    return out.reshape(rows, d)


def body(sizes, *arrays):
    rows = arrays[0].shape[0]
    heads = arrays[12].shape[0]
    sinks = arrays[14].shape[0]
    n = sizes["sp"]
    fits = (
        sizes["grp"] == 2
        and sizes["tp"] == 2 * CORES
        and n == 2 * CORES
        and heads == CORES
        and sinks == 2 * CORES
        and arrays[6].shape[1] == CORES * HD
        and rows == 2 * WINDOW
    )
    if fits:
        return transposed(n, *arrays)
    return on_device(*arrays)


def solution(mesh):
    return jax.shard_map(
        functools.partial(body, dict(mesh.shape)),
        mesh=mesh,
        in_specs=(
            P(("grp", "sp"), None),
            P(),
            P("sp", "tp"),
            P("sp", "tp"),
            P("sp", "tp"),
            P("sp", "tp"),
            P("sp", "tp"),
            P("sp", "tp"),
            P(),
            P(),
            P(),
            P(),
            P("tp"),
            P(),
            P("tp"),
            P("tp", None),
            P("tp", None),
        ),
        out_specs=P(("grp", "sp"), None),
        check_vma=False,
    )
```
